512 devices in a mesh: sp: 64 (over z, y), tp: 8 (over x, core).
Axes of the slice: x: 4, y: 4, z: 16, core: 2. Of those that a mesh axis runs over, the one named last changes fastest.
Arguments:
- tokens: bfloat16 [8192, 1024], P('sp', 'tp'), may hold values from -6 to 6
- norm_gain: float32 [1024], P('tp'), may hold values from 0.1 to 1.9
- query_weight: bfloat16 [1024, 1024], P('sp', 'tp'), may hold values from -0.1875 to 0.1875
- key_weight: bfloat16 [1024, 512], P('sp', 'tp'), may hold values from -0.1875 to 0.1875
- value_weight: bfloat16 [1024, 512], P('sp', 'tp'), may hold values from -0.1875 to 0.1875
- conv_in_weight: bfloat16 [1024, 1024], P('sp', 'tp'), may hold values from -0.1875 to 0.1875
- pre_weight: bfloat16 [1024, 1024], P('sp', 'tp'), may hold values from -0.1875 to 0.1875
- post_weight: bfloat16 [1024, 1024], P('sp', 'tp'), may hold values from -0.1875 to 0.1875
- attn_gate_weight: bfloat16 [1024, 1024], P('sp', 'tp'), may hold values from -0.1875 to 0.1875
- conv_gate_weight: bfloat16 [1024, 1024], P('sp', 'tp'), may hold values from -0.1875 to 0.1875
- sink_logit: float32 [16], P('tp'), may hold values from 1 to 5
- conv_taps: float32 [3, 1024], P(None, 'tp'), may hold values from -3 to 3
- attn_out_weight: bfloat16 [1024, 1024], P('tp', 'sp'), may hold values from -1 to 1
- conv_out_weight: bfloat16 [1024, 1024], P('tp', 'sp'), may hold values from -0.1875 to 0.1875
Outputs:
- merged: bfloat16 [8192, 1024], P('sp', 'tp')
The draws below stay inside these ranges and needn't reach their ends.
All inputs are finite; a program needn't handle non-finite values.
Results may differ from the reference program's by a relative error of at most 0.003.
Values may be sent and summed in bfloat16 or wider, within the bound.
No kernel may reach another device: no remote copies, remote signals or barrier semaphores. Data moves between devices by JAX's collectives and lax.ppermute only.
A program may use at most 64 MiB of HBM per device.

```python
import jax
import jax.numpy as jnp
from jax import lax

D = 1024
Q_HEADS = 16
KV_HEADS = 8
HEAD_DIM = 64
WINDOW = 64
TOK_DEV = 128
GROUP = 2
ATTN_WIDTH = 1024
KV_WIDTH = 512
TOKENS = 8192


def steps_of(rng, extent, pieces, low, top_value):
    level, own = 1.0, jax.random.fold_in(rng, 6)
    for position, parts in pieces:
        heights = jnp.exp(jax.random.uniform(jax.random.fold_in(own, position), (parts,), jnp.float32, low / len(pieces), top_value / len(pieces)))
        level = level * jnp.repeat(heights, extent[position] // parts).reshape([-1 if axis == position else 1 for axis in range(len(extent))])
    return level


def centred(rng, shape, width, limit, shards=(), kind=jnp.bfloat16):
    result = jax.random.normal(rng, shape, jnp.float32) * width
    if len(shards) > 0:
        result = steps_of(rng, shape, shards, -0.22, 0.18) * result
    return jnp.clip(result, min=-limit, max=limit).astype(kind)


def setup_inputs(seed: int = 0) -> dict:
    arg_keys = jax.random.split(jax.random.key(seed), 15)
    return {
        "tokens": centred(arg_keys[0], (TOKENS, D), 1.0, 6.0, ((0, 64), (1, 8))),
        "norm_gain": jnp.clip(1.0 + 0.18 * jax.random.normal(arg_keys[1], (D,), jnp.float32), 0.1, 1.9),
        "query_weight": centred(arg_keys[2], (D, ATTN_WIDTH), D ** -0.5, 0.1875, ((0, 64), (1, 8))),
        "key_weight": centred(arg_keys[3], (D, KV_WIDTH), D ** -0.5, 0.1875, ((0, 64), (1, 8))),
        "value_weight": centred(arg_keys[4], (D, KV_WIDTH), D ** -0.5, 0.1875, ((0, 64), (1, 8))),
        "conv_in_weight": centred(arg_keys[5], (D, D), D ** -0.5, 0.1875, ((0, 64), (1, 8))),
        "pre_weight": centred(arg_keys[6], (D, D), D ** -0.5, 0.1875, ((0, 64), (1, 8))),
        "post_weight": centred(arg_keys[7], (D, D), D ** -0.5, 0.1875, ((0, 64), (1, 8))),
        "attn_gate_weight": centred(arg_keys[8], (D, D), D ** -0.5, 0.1875, ((0, 64), (1, 8))),
        "conv_gate_weight": centred(arg_keys[9], (D, D), D ** -0.5, 0.1875, ((0, 64), (1, 8))),
        "sink_logit": jnp.clip(1.0 + 4.0 * jax.random.uniform(arg_keys[10], (Q_HEADS,), jnp.float32) ** steps_of(arg_keys[10], (Q_HEADS,), ((0, 8),), -0.2, 0.2), 1.0, 5.0),
        "conv_taps": centred(arg_keys[11], (3, D), 0.577, 3.0, ((1, 8),), jnp.float32),
        "attn_out_weight": centred(arg_keys[12], (ATTN_WIDTH, D), (ATTN_WIDTH // 32) ** -0.5, 1.0, ((0, 8), (1, 64))),
        "conv_out_weight": centred(arg_keys[13], (D, D), D ** -0.5, 0.1875, ((0, 8), (1, 64))),
    }


epsilon = 1e-06
negative = -1e+30

def window_mix(queries, key_rows, value_rows, sink_cols, first, seq_total):
    score_scale = queries.shape[-1] ** (-0.5)
    scores = jnp.einsum('qhgd,khd->hgqk', queries, key_rows, precision=lax.Precision.HIGHEST) * score_scale
    qpos = first + jnp.arange(queries.shape[0], dtype=jnp.int32)
    kpos = first - WINDOW + jnp.arange(key_rows.shape[0], dtype=jnp.int32)
    allowed = (jnp.abs(qpos[:, None] - kpos[None, :]) <= WINDOW) & (kpos >= 0)[None, :] & (kpos < seq_total)[None, :]
    scores = jnp.where(allowed, scores, negative)
    column = jnp.broadcast_to(sink_cols[:, :, None, None], scores.shape[:-1] + (1,))
    weights_soft = jax.nn.softmax(jnp.concatenate([scores, column], axis=-1), axis=-1)[..., :-1]
    return jnp.einsum('hgqk,khd->qhgd', weights_soft, value_rows, precision=lax.Precision.HIGHEST)

def attention(queries, key_rows, value_rows, sink_logit):
    padding = ((WINDOW, WINDOW), (0, 0))
    key_pad = jnp.pad(key_rows.astype(jnp.float32), padding)
    value_pad = jnp.pad(value_rows.astype(jnp.float32), padding)
    span_rows = TOK_DEV + 2 * WINDOW
    sink_cols = sink_logit.reshape(KV_HEADS, GROUP)

    def block(block_index):
        first = block_index * TOK_DEV
        q_block = lax.dynamic_slice_in_dim(queries, first, TOK_DEV, 0).astype(jnp.float32)
        q_block = q_block.reshape(TOK_DEV, KV_HEADS, GROUP, HEAD_DIM)
        k_block = lax.dynamic_slice_in_dim(key_pad, first, span_rows, 0).reshape(span_rows, KV_HEADS, HEAD_DIM)
        v_block = lax.dynamic_slice_in_dim(value_pad, first, span_rows, 0).reshape(span_rows, KV_HEADS, HEAD_DIM)
        mixed_rows = window_mix(q_block, k_block, v_block, sink_cols, first, TOKENS)
        return mixed_rows.reshape(TOK_DEV, ATTN_WIDTH)
    blocks_out = lax.map(block, jnp.arange(TOKENS // TOK_DEV, dtype=jnp.int32))
    return blocks_out.reshape(TOKENS, ATTN_WIDTH).astype(jnp.bfloat16)

def reference(tokens, norm_gain, query_weight, key_weight, value_weight, conv_in_weight, pre_weight, post_weight, attn_gate_weight, conv_gate_weight, sink_logit, conv_taps, attn_out_weight, conv_out_weight):
    widened = tokens.astype(jnp.float32)
    mean_sq = lax.optimization_barrier(jnp.mean(widened * widened, axis=1, keepdims=True))
    normed = (widened * lax.rsqrt(mean_sq + epsilon) * norm_gain[None, :]).astype(jnp.bfloat16)

    def project(weight):
        return jnp.dot(normed, weight, preferred_element_type=jnp.float32)
    queries = project(query_weight).astype(jnp.bfloat16)
    key_rows = project(key_weight).astype(jnp.bfloat16)
    value_rows = project(value_weight).astype(jnp.bfloat16)
    conv_in = project(conv_in_weight).astype(jnp.bfloat16)
    pre_gate = project(pre_weight).astype(jnp.bfloat16)
    post_gate = project(post_weight).astype(jnp.bfloat16)
    attn_gate = project(attn_gate_weight)
    conv_gate = project(conv_gate_weight)
    attended = attention(queries, key_rows, value_rows, sink_logit)
    conv_mix = (pre_gate.astype(jnp.float32) * conv_in.astype(jnp.float32)).astype(jnp.bfloat16)
    padded = jnp.pad(conv_mix.astype(jnp.float32), ((1, 1), (0, 0)))
    convolved = conv_taps[0][None, :] * padded[:-2] + conv_taps[1][None, :] * padded[1:-1] + conv_taps[2][None, :] * padded[2:]
    conv_out = (post_gate.astype(jnp.float32) * convolved).astype(jnp.bfloat16)
    branch_attn = jnp.dot(attended, attn_out_weight, preferred_element_type=jnp.float32)
    branch_conv = jnp.dot(conv_out, conv_out_weight, preferred_element_type=jnp.float32)
    return (jax.nn.sigmoid(attn_gate) * branch_attn + jax.nn.sigmoid(conv_gate) * branch_conv).astype(jnp.bfloat16)
```

```python
import functools

import jax
import jax.numpy as jnp
from jax import lax
from jax.experimental import pallas as pl
from jax.experimental.pallas import tpu as pltpu
from jax.sharding import Mesh
from jax.sharding import PartitionSpec as P

ZN, YN, XN, CN = 16, 4, 4, 2
TPN = XN * CN
PLANE = YN * TPN
HALF = 64
WINDOW = 64
LANES = 128
TOK = 128
ROWS = YN * TOK + 2 * WINDOW
SLOT = TOK + WINDOW
FEATURES = TPN * LANES
EPSILON = 1e-06
NEGATIVE = -1e30
F32 = jnp.float32
BF16 = jnp.bfloat16


def nt_dot(a, b):
    return lax.dot_general(a, b, (((1,), (1,)), ((), ())), preferred_element_type=F32)


def nn_dot(a, b):
    return jnp.dot(a, b, preferred_element_type=F32)


def turned(block):
    return jnp.concatenate([block[:, HALF:], block[:, :HALF]], axis=1)


def pack_kernel(tok, q, k, v, ci, pre, post, ag, cg, wa, wc, wy_out, halo_out):
    y = lax.axis_index("y")
    for role in range(YN):
        half = slice(HALF * (role % 2), HALF * (role % 2) + HALF)
        first = (q[:, half], k[...], v[...]) if role < 2 else (ci[:, half], pre[:, half], post[:, half])
        out_weight = wa if role < 2 else wc
        columns = first + (ag[:, :HALF], ag[:, HALF:], cg[:, :HALF], cg[:, HALF:], out_weight[:, half])
        for pair in range(4):
            wy_out[role, 16 * pair : 16 * pair + 16, :] = jnp.concatenate(columns[2 * pair : 2 * pair + 2], axis=1)
    halo_out[...] = jnp.where(y == YN - 1, tok[TOK - WINDOW :, :], tok[:WINDOW, :])


def spread_kernel(tok, halo, gain, out):
    y = lax.axis_index("y")
    g = gain[...]
    high = g.astype(BF16)
    rest = g - high.astype(F32)
    middle = rest.astype(BF16)
    low = (rest - middle.astype(F32)).astype(BF16)
    row = lax.broadcasted_iota(jnp.int32, (WINDOW, LANES), 0)
    parts = [jnp.broadcast_to(part.astype(F32), (WINDOW, LANES)) for part in (high, middle, low)]
    gains = jnp.where(row == 0, parts[0], jnp.where(row == 1, parts[1], jnp.where(row == 2, parts[2], 0.0)))
    slot = jnp.where(y == 1, gains.astype(BF16), halo[...])
    block = tok[...]
    for peer in range(PLANE):
        out[peer, :TOK, :] = block
        out[peer, TOK:, :] = slot


def mix_kernel(t, w, taps, sink, out, own, n_scr, p_scr):
    y = lax.axis_index("y")
    z = lax.axis_index("z")
    gains = []
    for tp in range(TPN):
        r = t[TPN + tp, TOK : TOK + 16, :].astype(F32)
        gains.append(r[0:1] + r[1:2] + r[2:3])
    segments = [(0, 0, TOK, WINDOW)]
    segments += [(WINDOW + TOK * b, b, 0, TOK) for b in range(YN)]
    segments += [(WINDOW + TOK * YN, YN - 1, TOK, WINDOW)]
    for at, b, start, count in segments:
        total = jnp.zeros((count, LANES), F32)
        for tp in range(TPN):
            x = t[b * TPN + tp, start : start + count, :].astype(F32)
            total = total + x * x
        scale = lax.rsqrt(jnp.sum(total, axis=1, keepdims=True) / FEATURES + EPSILON)
        for tp in range(TPN):
            x = t[b * TPN + tp, start : start + count, :].astype(F32)
            n_scr[at : at + count, LANES * tp : LANES * (tp + 1)] = (x * scale * gains[tp]).astype(BF16)
    own[...] = n_scr[pl.ds(pl.multiple_of(WINDOW + TOK * y, WINDOW), TOK), :]
    weight = jnp.concatenate(
        [w[:, :, 16 * pair : 16 * pair + 16, :].reshape(FEATURES, LANES) for pair in range(2)], axis=1
    )
    p_scr[...] = nn_dot(n_scr[...], weight)
    left = lax.broadcasted_iota(jnp.int32, (TOK, LANES), 1) < HALF

    def send(b, mixed):
        for tp in range(TPN):
            columns = w[2 * tp : 2 * tp + 2, :, 48:64, :].reshape(LANES, LANES)
            out[b * TPN + tp] = jnp.where(left, mixed, columns)

    @pl.when(y < 2)
    def _():
        logit = jnp.where(y == 0, sink[0], sink[1])
        span = TOK + 2 * WINDOW
        i = lax.broadcasted_iota(jnp.int32, (TOK, span), 0)
        j = lax.broadcasted_iota(jnp.int32, (TOK, span), 1)
        near = jnp.abs(i + WINDOW - j) <= WINDOW
        for b in range(YN):
            q = p_scr[WINDOW + TOK * b : WINDOW + TOK * (b + 1), :HALF].astype(BF16)
            k = p_scr[TOK * b : TOK * b + span, HALF:LANES].astype(BF16)
            v = p_scr[TOK * b : TOK * b + span, LANES:].astype(BF16)
            scores = nt_dot(q, k) * (HALF**-0.5)
            key = (z * YN + b) * TOK - WINDOW + j
            allowed = near & (key >= 0) & (key < ZN * YN * TOK)
            scores = jnp.where(allowed, scores, NEGATIVE)
            top = jnp.maximum(jnp.max(scores, axis=1, keepdims=True), logit)
            e = jnp.exp(scores - top)
            share = jnp.sum(e, axis=1, keepdims=True) + jnp.exp(logit - top)
            e = e / share
            high = e.astype(BF16)
            low = (e - high.astype(F32)).astype(BF16)
            send(b, (nn_dot(high, v) + nn_dot(low, v)).astype(BF16))

    @pl.when(y >= 2)
    def _():
        t3 = jnp.where(y == YN - 1, turned(taps[...]), taps[...])
        c = p_scr[:, :LANES].astype(BF16).astype(F32)
        p_scr[:, :LANES] = (c * turned(c)).astype(BF16).astype(F32)
        for b in range(YN):
            at = WINDOW + TOK * b
            before = p_scr[at - 1 : at - 1 + TOK, :LANES]
            here = p_scr[at : at + TOK, :LANES]
            after = p_scr[at + 1 : at + 1 + TOK, :LANES]
            post = p_scr[at : at + TOK, LANES:].astype(BF16).astype(F32)
            send(b, (post * (t3[0:1] * before + t3[1:2] * here + t3[2:3] * after)).astype(BF16))


def gate_kernel(own, w, out):
    weight = jnp.concatenate(
        [w[:, :, 16 * pair : 16 * pair + 16, :].reshape(FEATURES, LANES) for pair in range(1, 4)], axis=1
    )
    g = nn_dot(own[...], weight)
    out[...] = jax.nn.sigmoid(g[:, HALF : HALF + 2 * LANES])


def final_kernel(m, gates, out):
    left = lax.broadcasted_iota(jnp.int32, (TOK, LANES), 1) < HALF
    branches = []
    for branch in range(2):
        mixed, columns = [], []
        for tp in range(TPN):
            a = m[(2 * branch) * TPN + tp]
            b = m[(2 * branch + 1) * TPN + tp]
            mixed.append(jnp.where(left, a, turned(b)))
            columns.append(jnp.where(left, turned(a), b))
        branches.append(nt_dot(jnp.concatenate(mixed, axis=1), jnp.concatenate(columns, axis=1)))
    out[...] = (gates[:, :LANES] * branches[0] + gates[:, LANES:] * branches[1]).astype(BF16)


VM = pl.BlockSpec(memory_space=pltpu.VMEM)
SM = pl.BlockSpec(memory_space=pltpu.SMEM)


def shaped(shape, kind=BF16):
    return jax.ShapeDtypeStruct(shape, kind)


def on_device(tok, gain, q, k, v, ci, pre, post, ag, cg, sink, taps, wa, wc):
    plane = ("y", "x", "c")
    wy, halo = pl.pallas_call(
        pack_kernel,
        out_shape=(shaped((YN, 64, LANES)), shaped((WINDOW, LANES))),
        in_specs=[VM] * 11,
        out_specs=(VM, VM),
        name="pack",
    )(tok, q, k, v, ci, pre, post, ag, cg, wa.T, wc.T)
    edges = [(YN * z + YN - 1, YN * z + YN) for z in range(ZN - 1)]
    halo = lax.ppermute(halo, ("z", "y"), edges + [(b, a) for a, b in edges])
    wy = lax.all_to_all(wy, "y", 0, 0, tiled=True)
    spread = pl.pallas_call(
        spread_kernel,
        out_shape=shaped((PLANE, SLOT, LANES)),
        in_specs=[VM] * 3,
        out_specs=VM,
        name="spread",
    )(tok, halo, gain.reshape(1, LANES))
    gathered_tok = lax.all_to_all(spread, plane, 0, 0, tiled=True)
    w = lax.all_gather(wy.reshape(YN * 64, LANES), "z", axis=0, tiled=True).reshape(ZN, YN, 64, LANES)
    message, own = pl.pallas_call(
        mix_kernel,
        out_shape=(shaped((PLANE, TOK, LANES)), shaped((TOK, FEATURES))),
        in_specs=[VM, VM, VM, SM],
        out_specs=(VM, VM),
        scratch_shapes=[pltpu.VMEM((ROWS, FEATURES), BF16), pltpu.VMEM((ROWS, 2 * LANES), F32)],
        name="mix",
    )(gathered_tok, w, taps, sink)
    message = lax.all_to_all(message, plane, 0, 0, tiled=True)
    gates = pl.pallas_call(
        gate_kernel,
        out_shape=shaped((TOK, 2 * LANES), F32),
        in_specs=[VM] * 2,
        out_specs=VM,
        name="gate",
    )(own, w)
    return pl.pallas_call(
        final_kernel,
        out_shape=shaped((TOK, LANES)),
        in_specs=[VM] * 2,
        out_specs=VM,
        name="final",
    )(message, gates)


def solution(mesh):
    finer = Mesh(mesh.devices.reshape(ZN, YN, XN, CN), ("z", "y", "x", "c"))
    sp, tp = ("z", "y"), ("x", "c")
    rows = P(sp, tp)
    columns = P(tp, sp)
    return jax.shard_map(
        on_device,
        mesh=finer,
        in_specs=(rows, P(tp)) + (rows,) * 8 + (P(tp), P(None, tp), columns, columns),
        out_specs=rows,
        check_vma=False,
    )
```

```python
import jax
import jax.numpy as jnp
from jax import lax
from jax.experimental import pallas as pl
from jax.experimental.pallas import tpu as pltpu
from jax.sharding import Mesh
from jax.sharding import PartitionSpec as P


ZN, YN, XN, CN = 16, 4, 4, 2
TPN = XN * CN
PLANE = YN * TPN
HALF = 64
WINDOW = 64
LANES = 128
TOK = 128
ROWS = YN * TOK + 2 * WINDOW
SLOT = TOK + WINDOW
FEATURES = TPN * LANES
EPSILON = 1e-06
NEGATIVE = -1e30
F32 = jnp.float32
BF16 = jnp.bfloat16


def nt_dot(a, b):
    return lax.dot_general(a, b, (((1,), (1,)), ((), ())), preferred_element_type=F32)


def nn_dot(a, b):
    return jnp.dot(a, b, preferred_element_type=F32)


def turned(block):
    return jnp.concatenate([block[:, HALF:], block[:, :HALF]], axis=1)


def pack_kernel(tok, gain, q, k, v, ci, pre, post, ag, cg, wa, wc, wy_out, halo_out, base_out):
    y = lax.axis_index("y")
    for role in range(YN):
        half = slice(HALF * (role % 2), HALF * (role % 2) + HALF)
        first = (q, k, v) if role < 2 else (ci, pre, post)
        first = [block[:, half] if block.shape[1] == LANES else block[...] for block in first]
        gate, out_weight = (ag, wa) if role < 2 else (cg, wc)
        wy_out[role, 0:16, :] = jnp.concatenate(first[:2], axis=1)
        wy_out[role, 16:32, :] = jnp.concatenate([first[2], gate[:, half]], axis=1)
        rows = out_weight[:, half].astype(F32)
        wy_out[role, 32:40, :] = jnp.concatenate([rows[:8], rows[8:]], axis=1).astype(BF16)
    halo_out[...] = jnp.where(y == YN - 1, tok[TOK - WINDOW :, :], tok[:WINDOW, :])
    g = gain[...]
    high = g.astype(BF16)
    rest = g - high.astype(F32)
    middle = rest.astype(BF16)
    low = (rest - middle.astype(F32)).astype(BF16)
    row = lax.broadcasted_iota(jnp.int32, (WINDOW, LANES), 0)
    parts = [jnp.broadcast_to(part.astype(F32), (WINDOW, LANES)) for part in (high, middle, low)]
    gains = jnp.where(row == 0, parts[0], jnp.where(row == 1, parts[1], jnp.where(row == 2, parts[2], 0.0)))
    base_out[:TOK, :] = tok[...]
    base_out[TOK:, :] = gains.astype(BF16)


def spread_kernel(base, halo, out):
    y = lax.axis_index("y")
    slot = jnp.where(y == 1, base[TOK:, :], halo[...])
    block = base[:TOK, :]
    for peer in range(PLANE):
        out[peer, :TOK, :] = block
        out[peer, TOK:, :] = slot


def mix_kernel(t, w, taps, sink, out, gates, n_scr, p_scr):
    y = lax.axis_index("y")
    z = lax.axis_index("z")
    gains = []
    for tp in range(TPN):
        r = t[TPN + tp, TOK : TOK + 16, :].astype(F32)
        gains.append(r[0:1] + r[1:2] + r[2:3])
    segments = [(0, 0, TOK, WINDOW)]
    segments += [(WINDOW + TOK * b, b, 0, TOK) for b in range(YN)]
    segments += [(WINDOW + TOK * YN, YN - 1, TOK, WINDOW)]
    for at, b, start, count in segments:
        total = jnp.zeros((count, LANES), F32)
        for tp in range(TPN):
            x = t[b * TPN + tp, start : start + count, :].astype(F32)
            total = total + x * x
        scale = lax.rsqrt(jnp.sum(total, axis=1, keepdims=True) / FEATURES + EPSILON)
        for tp in range(TPN):
            x = t[b * TPN + tp, start : start + count, :].astype(F32)
            n_scr[at : at + count, LANES * tp : LANES * (tp + 1)] = (x * scale * gains[tp]).astype(BF16)
    weight = jnp.concatenate(
        [w[:, :, 16 * pair : 16 * pair + 16, :].reshape(FEATURES, LANES) for pair in range(2)], axis=1
    )
    p_scr[...] = nn_dot(n_scr[...], weight)
    left = lax.broadcasted_iota(jnp.int32, (TOK, LANES), 1) < HALF
    for b in range(YN):
        at = WINDOW + TOK * b
        gates[b] = jnp.where(left[:HALF], turned(p_scr[at : at + HALF, LANES:]), p_scr[at + HALF : at + TOK, LANES:])

    def send(b, mixed):
        for tp in range(TPN):
            rows = w[2 * tp : 2 * tp + 2, :, 32:40, :].astype(F32).reshape(TPN, 8, LANES)
            rows = jnp.stack([turned(rows.reshape(HALF, LANES)).reshape(TPN, 8, LANES), rows], axis=1)
            out[b * TPN + tp] = jnp.where(left, mixed, rows.reshape(LANES, LANES).astype(BF16))

    @pl.when(y < 2)
    def _():
        logit = jnp.where(y == 0, sink[0], sink[1])
        span = TOK + 2 * WINDOW
        i = lax.broadcasted_iota(jnp.int32, (TOK, span), 0)
        j = lax.broadcasted_iota(jnp.int32, (TOK, span), 1)
        near = jnp.abs(i + WINDOW - j) <= WINDOW
        for b in range(YN):
            q = p_scr[WINDOW + TOK * b : WINDOW + TOK * (b + 1), :HALF].astype(BF16)
            k = p_scr[TOK * b : TOK * b + span, HALF:LANES].astype(BF16)
            v = p_scr[TOK * b : TOK * b + span, LANES:].astype(BF16)
            scores = nt_dot(q, k) * (HALF**-0.5)
            key = (z * YN + b) * TOK - WINDOW + j
            allowed = near & (key >= 0) & (key < ZN * YN * TOK)
            scores = jnp.where(allowed, scores, NEGATIVE)
            top = jnp.maximum(jnp.max(scores, axis=1, keepdims=True), logit)
            e = jnp.exp(scores - top)
            share = jnp.sum(e, axis=1, keepdims=True) + jnp.exp(logit - top)
            e = e / share
            high = e.astype(BF16)
            low = (e - high.astype(F32)).astype(BF16)
            send(b, (nn_dot(high, v) + nn_dot(low, v)).astype(BF16))

    @pl.when(y >= 2)
    def _():
        t3 = jnp.where(y == YN - 1, turned(taps[...]), taps[...])
        c = p_scr[:, :LANES].astype(BF16).astype(F32)
        p_scr[:, :LANES] = (c * turned(c)).astype(BF16).astype(F32)
        for b in range(YN):
            at = WINDOW + TOK * b
            before = p_scr[at - 1 : at - 1 + TOK, :LANES]
            here = p_scr[at : at + TOK, :LANES]
            after = p_scr[at + 1 : at + 1 + TOK, :LANES]
            post = p_scr[at : at + TOK, LANES:].astype(BF16).astype(F32)
            send(b, (post * (t3[0:1] * before + t3[1:2] * here + t3[2:3] * after)).astype(BF16))


def joined(a, b, left):
    return jnp.where(left, a, turned(b)), jnp.where(left, turned(a), b)


def gate_kernel(g, out):
    y = lax.axis_index("y")
    left = lax.broadcasted_iota(jnp.int32, (HALF, LANES), 1) < HALF
    for branch in range(2):
        both = joined(g[2 * branch, y], g[2 * branch + 1, y], left)
        out[branch] = jax.nn.sigmoid(jnp.concatenate(both, axis=0))


def final_kernel(m, gates, out):
    left = lax.broadcasted_iota(jnp.int32, (TOK, LANES), 1) < HALF
    total = jnp.zeros((TOK, LANES), F32)
    for branch in range(2):
        mixed, columns = [], []
        for tp in range(TPN):
            both = joined(m[(2 * branch) * TPN + tp], m[(2 * branch + 1) * TPN + tp], left)
            mixed.append(both[0])
            columns.append(both[1])
        value = nt_dot(jnp.concatenate(mixed, axis=1), jnp.concatenate(columns, axis=1))
        total = total + gates[branch] * value
    out[...] = total.astype(BF16)


VM = pl.BlockSpec(memory_space=pltpu.VMEM)
SM = pl.BlockSpec(memory_space=pltpu.SMEM)


def shaped(shape, kind=BF16):
    return jax.ShapeDtypeStruct(shape, kind)


def call(kernel, outs, args, specs=None, scratch=(), limit=8):
    return pl.pallas_call(
        kernel,
        out_shape=outs,
        in_specs=specs or [VM] * len(args),
        out_specs=jax.tree.map(lambda _: VM, outs),
        scratch_shapes=list(scratch),
        compiler_params=pltpu.CompilerParams(vmem_limit_bytes=limit * 2**20),
    )(*args)


def on_device(tok, gain, q, k, v, ci, pre, post, ag, cg, sink, taps, wa, wc):
    plane = ("y", "x", "c")
    wy, halo, base = call(
        pack_kernel,
        (shaped((YN, 40, LANES)), shaped((WINDOW, LANES)), shaped((SLOT, LANES))),
        (tok, gain.reshape(1, LANES), q, k, v, ci, pre, post, ag, cg, wa.T, wc.T),
        limit=60,
    )
    edges = [(YN * z + YN - 1, YN * z + YN) for z in range(ZN - 1)]
    halo = lax.ppermute(halo, ("z", "y"), edges + [(b, a) for a, b in edges])
    wy = lax.all_to_all(wy, "y", 0, 0, tiled=True)
    spread = call(spread_kernel, shaped((PLANE, SLOT, LANES)), (base, halo))
    gathered_tok = lax.all_to_all(spread, plane, 0, 0, tiled=True)
    w = lax.all_gather(wy.reshape(YN * 40, LANES), "z", axis=0, tiled=True).reshape(ZN, YN, 40, LANES)
    message, gates = call(
        mix_kernel,
        (shaped((PLANE, TOK, LANES)), shaped((YN, HALF, LANES), F32)),
        (gathered_tok, w, taps, sink),
        [VM, VM, VM, SM],
        [pltpu.VMEM((ROWS, FEATURES), BF16), pltpu.VMEM((ROWS, 2 * LANES), F32)],
        20,
    )
    message = lax.all_to_all(message, plane, 0, 0, tiled=True)
    gates = lax.all_gather(gates, "y")
    gates = call(gate_kernel, shaped((2, TOK, LANES), F32), (gates,))
    return call(final_kernel, shaped((TOK, LANES)), (message, gates))


def solution(mesh):
    finer = Mesh(mesh.devices.reshape(ZN, YN, XN, CN), ("z", "y", "x", "c"))
    sp, tp = ("z", "y"), ("x", "c")
    rows = P(sp, tp)
    columns = P(tp, sp)
    return jax.shard_map(
        on_device,
        mesh=finer,
        in_specs=(rows, P(tp)) + (rows,) * 8 + (P(tp), P(None, tp), columns, columns),
        out_specs=rows,
        check_vma=False,
    )
```

```python
import jax
import jax.numpy as jnp
from jax import lax
from jax.experimental import pallas as pl
from jax.experimental.pallas import tpu as pltpu
from jax.sharding import Mesh
from jax.sharding import PartitionSpec as P


ZN, YN, XN, CN = 16, 4, 4, 2
TPN = XN * CN
PLANE = YN * TPN
HALF = 64
WINDOW = 64
LANES = 128
TOK = 128
ROWS = YN * TOK
SLOT = TOK + 8
FEATURES = TPN * LANES
EPSILON = 1e-06
NEGATIVE = -1e30
F32 = jnp.float32
BF16 = jnp.bfloat16


def nt_dot(a, b):
    return lax.dot_general(a, b, (((1,), (1,)), ((), ())), preferred_element_type=F32)


def nn_dot(a, b):
    return jnp.dot(a, b, preferred_element_type=F32)


def turned(block):
    return jnp.concatenate([block[:, HALF:], block[:, :HALF]], axis=1)


def pack_kernel(q, k, v, ci, pre, post, ag, cg, wa, wc, wy_out):
    for role in range(YN):
        half = slice(HALF * (role % 2), HALF * (role % 2) + HALF)
        first = (q, k, v) if role < 2 else (ci, pre, post)
        first = [block[:, half] if block.shape[1] == LANES else block[...] for block in first]
        gate, out_weight = (ag, wa) if role < 2 else (cg, wc)
        wy_out[role, 0:16, :] = jnp.concatenate(first[:2], axis=1)
        wy_out[role, 16:32, :] = jnp.concatenate([first[2], gate[:, half]], axis=1)
        rows = out_weight[:, half].astype(F32)
        wy_out[role, 32:40, :] = jnp.concatenate([rows[:8], rows[8:]], axis=1).astype(BF16)


def spread_kernel(tok, gain, out):
    g = gain[...]
    high = g.astype(BF16)
    rest = g - high.astype(F32)
    middle = rest.astype(BF16)
    low = (rest - middle.astype(F32)).astype(BF16)
    row = lax.broadcasted_iota(jnp.int32, (8, LANES), 0)
    parts = [jnp.broadcast_to(part.astype(F32), (8, LANES)) for part in (high, middle, low)]
    gains = jnp.where(row == 0, parts[0], jnp.where(row == 1, parts[1], jnp.where(row == 2, parts[2], 0.0)))
    gains = gains.astype(BF16)
    block = tok[...]
    for peer in range(PLANE):
        out[peer, :TOK, :] = block
        out[peer, TOK:, :] = gains


def project_kernel(t, w, p, up, down, gate_0, gate_1, gate_2, gate_3, n_scr, g_scr):
    y = lax.axis_index("y")
    gains = []
    for tp in range(TPN):
        r = t[tp, TOK:, :].astype(F32)
        gains.append(r[0:1] + r[1:2] + r[2:3])
    for b in range(YN):
        total = jnp.zeros((TOK, LANES), F32)
        for tp in range(TPN):
            x = t[b * TPN + tp, :TOK, :].astype(F32)
            total = total + x * x
        scale = lax.rsqrt(jnp.sum(total, axis=1, keepdims=True) / FEATURES + EPSILON)
        for tp in range(TPN):
            x = t[b * TPN + tp, :TOK, :].astype(F32)
            n_scr[TOK * b : TOK * (b + 1), LANES * tp : LANES * (tp + 1)] = (x * scale * gains[tp]).astype(BF16)
    weight = jnp.concatenate(
        [w[:, :, 16 * pair : 16 * pair + 16, :].reshape(FEATURES, LANES) for pair in range(2)], axis=1
    )
    value = nn_dot(n_scr[...], weight)
    p[...] = value.astype(BF16)
    left = lax.broadcasted_iota(jnp.int32, (HALF, LANES), 1) < HALF
    for out, at in ((up, ROWS - WINDOW), (down, 0)):
        mixed = jnp.where(left & (y < 2), p[at : at + WINDOW, LANES:], p[at : at + WINDOW, :LANES])
        out[...] = mixed
    for b in range(YN):
        at = TOK * b
        g_scr[b] = jnp.where(left, turned(value[at : at + HALF, LANES:]), value[at + HALF : at + TOK, LANES:])
    for k, out in enumerate((gate_0, gate_1, gate_2, gate_3)):
        out[...] = g_scr[lax.rem(y + k, YN)]


def mix_kernel(p, before, after, w, taps, sink, out, c_scr):
    y = lax.axis_index("y")
    z = lax.axis_index("z")
    left = lax.broadcasted_iota(jnp.int32, (TOK, LANES), 1) < HALF

    def send(b, mixed):
        for tp in range(TPN):
            rows = w[2 * tp : 2 * tp + 2, :, 32:40, :].astype(F32).reshape(TPN, 8, LANES)
            rows = jnp.stack([turned(rows.reshape(HALF, LANES)).reshape(TPN, 8, LANES), rows], axis=1)
            out[b * TPN + tp] = jnp.where(left, mixed, rows.reshape(LANES, LANES).astype(BF16))

    @pl.when(y < 2)
    def _():
        logit = jnp.where(y == 0, sink[0], sink[1])
        span = TOK + 2 * WINDOW
        i = lax.broadcasted_iota(jnp.int32, (TOK, span), 0)
        j = lax.broadcasted_iota(jnp.int32, (TOK, span), 1)
        near = jnp.abs(i + WINDOW - j) <= WINDOW
        keys = jnp.concatenate([before[:, HALF:], p[:, HALF:LANES], after[:, HALF:]], axis=0)
        values = jnp.concatenate([before[...], p[:, LANES:], after[...]], axis=0)
        for b in range(YN):
            q = p[TOK * b : TOK * (b + 1), :HALF]
            k = keys[TOK * b : TOK * b + span]
            v = values[TOK * b : TOK * b + span]
            scores = nt_dot(q, k) * (HALF**-0.5)
            key = (z * YN + b) * TOK - WINDOW + j
            allowed = near & (key >= 0) & (key < ZN * YN * TOK)
            scores = jnp.where(allowed, scores, NEGATIVE)
            top = jnp.maximum(jnp.max(scores, axis=1, keepdims=True), logit)
            e = jnp.exp(scores - top)
            share = jnp.sum(e, axis=1, keepdims=True) + jnp.exp(logit - top)
            e = e / share
            high = e.astype(BF16)
            low = (e - high.astype(F32)).astype(BF16)
            send(b, (nn_dot(high, v) + nn_dot(low, v)).astype(BF16))

    @pl.when(y >= 2)
    def _():
        t3 = jnp.where(y == YN - 1, turned(taps[...]), taps[...])

        def gated(block):
            wide = block.astype(F32)
            return (wide * turned(wide)).astype(BF16).astype(F32)

        c_scr[:WINDOW] = gated(before[...])
        c_scr[WINDOW : WINDOW + ROWS] = gated(p[:, :LANES])
        c_scr[WINDOW + ROWS :] = gated(after[...])
        for b in range(YN):
            at = WINDOW + TOK * b
            last = c_scr[at - 1 : at - 1 + TOK]
            here = c_scr[at : at + TOK]
            coming = c_scr[at + 1 : at + 1 + TOK]
            post = p[TOK * b : TOK * (b + 1), LANES:].astype(F32)
            send(b, (post * (t3[0:1] * last + t3[1:2] * here + t3[2:3] * coming)).astype(BF16))


def joined(a, b, left):
    return jnp.where(left, a, turned(b)), jnp.where(left, turned(a), b)


def gate_kernel(g_0, g_1, g_2, g_3, out, g_scr):
    y = lax.axis_index("y")
    for k, g in enumerate((g_0, g_1, g_2, g_3)):
        g_scr[k] = g[...]
    left = lax.broadcasted_iota(jnp.int32, (HALF, LANES), 1) < HALF
    for branch in range(2):
        parts = [g_scr[lax.rem(y + YN - source, YN)] for source in (2 * branch, 2 * branch + 1)]
        out[branch] = jax.nn.sigmoid(jnp.concatenate(joined(*parts, left), axis=0))


def final_kernel(m, gates, out):
    left = lax.broadcasted_iota(jnp.int32, (TOK, LANES), 1) < HALF
    total = jnp.zeros((TOK, LANES), F32)
    for branch in range(2):
        mixed, columns = [], []
        for tp in range(TPN):
            both = joined(m[(2 * branch) * TPN + tp], m[(2 * branch + 1) * TPN + tp], left)
            mixed.append(both[0])
            columns.append(both[1])
        value = nt_dot(jnp.concatenate(mixed, axis=1), jnp.concatenate(columns, axis=1))
        total = total + gates[branch] * value
    out[...] = total.astype(BF16)


VM = pl.BlockSpec(memory_space=pltpu.VMEM)
SM = pl.BlockSpec(memory_space=pltpu.SMEM)


def shaped(shape, kind=BF16):
    return jax.ShapeDtypeStruct(shape, kind)


def call(kernel, outs, args, specs=None, scratch=(), limit=8):
    return pl.pallas_call(
        kernel,
        out_shape=outs,
        in_specs=specs or [VM] * len(args),
        out_specs=jax.tree.map(lambda _: VM, outs),
        scratch_shapes=list(scratch),
        compiler_params=pltpu.CompilerParams(vmem_limit_bytes=limit * 2**20),
    )(*args)


def on_device(tok, gain, q, k, v, ci, pre, post, ag, cg, sink, taps, wa, wc):
    plane = ("y", "x", "c")
    wy = call(pack_kernel, shaped((YN, 40, LANES)), (q, k, v, ci, pre, post, ag, cg, wa.T, wc.T), limit=60)
    wy = lax.all_to_all(wy, "y", 0, 0, tiled=True)
    spread = call(spread_kernel, shaped((PLANE, SLOT, LANES)), (tok, gain.reshape(1, LANES)), limit=60)
    gathered_tok = lax.all_to_all(spread, plane, 0, 0, tiled=True)
    w = lax.all_gather(wy.reshape(YN * 40, LANES), "z", axis=0, tiled=True).reshape(ZN, YN, 40, LANES)
    gate_shape = shaped((HALF, LANES), F32)
    p, up, down, *gates = call(
        project_kernel,
        (shaped((ROWS, 2 * LANES)),) + (shaped((WINDOW, LANES)),) * 2 + (gate_shape,) * 4,
        (gathered_tok, w),
        scratch=[pltpu.VMEM((ROWS, FEATURES), BF16), pltpu.VMEM((YN, HALF, LANES), F32)],
        limit=20,
    )
    before = lax.ppermute(up, "z", [(z, z + 1) for z in range(ZN - 1)])
    after = lax.ppermute(down, "z", [(z + 1, z) for z in range(ZN - 1)])
    for k in range(1, YN):
        gates[k] = lax.ppermute(gates[k], "y", [(y, (y + k) % YN) for y in range(YN)])
    message = call(
        mix_kernel,
        shaped((PLANE, TOK, LANES)),
        (p, before, after, w, taps, sink),
        [VM] * 5 + [SM],
        [pltpu.VMEM((ROWS + 2 * WINDOW, LANES), F32)],
        16,
    )
    message = lax.all_to_all(message, plane, 0, 0, tiled=True)
    gates = call(gate_kernel, shaped((2, TOK, LANES), F32), gates, scratch=[pltpu.VMEM((YN, HALF, LANES), F32)])
    return call(final_kernel, shaped((TOK, LANES)), (message, gates))


def solution(mesh):
    finer = Mesh(mesh.devices.reshape(ZN, YN, XN, CN), ("z", "y", "x", "c"))
    sp, tp = ("z", "y"), ("x", "c")
    rows = P(sp, tp)
    columns = P(tp, sp)
    return jax.shard_map(
        on_device,
        mesh=finer,
        in_specs=(rows, P(tp)) + (rows,) * 8 + (P(tp), P(None, tp), columns, columns),
        out_specs=rows,
        check_vma=False,
    )
```

```python
import jax
import jax.numpy as jnp
from jax import lax
from jax.experimental import pallas as pl
from jax.experimental.pallas import tpu as pltpu
from jax.sharding import Mesh
from jax.sharding import PartitionSpec as P


ZN, YN, XN, CN = 16, 4, 4, 2
TPN = XN * CN
PLANE = YN * TPN
HALF = 64
WINDOW = 64
LANES = 128
TOK = 128
ROWS = YN * TOK + 2 * WINDOW
SLOT = TOK + WINDOW
FEATURES = TPN * LANES
EPSILON = 1e-06
NEGATIVE = -1e30
F32 = jnp.float32
BF16 = jnp.bfloat16


def nt_dot(a, b):
    return lax.dot_general(a, b, (((1,), (1,)), ((), ())), preferred_element_type=F32)


def nn_dot(a, b):
    return jnp.dot(a, b, preferred_element_type=F32)


def turned(block):
    return jnp.concatenate([block[:, HALF:], block[:, :HALF]], axis=1)


def pack_kernel(q, k, v, ci, pre, post, ag, cg, wa, wc, wy_out):
    for role in range(YN):
        half = slice(HALF * (role % 2), HALF * (role % 2) + HALF)
        first = (q, k, v) if role < 2 else (ci, pre, post)
        first = [block[:, half] if block.shape[1] == LANES else block[...] for block in first]
        gate, out_weight = (ag, wa) if role < 2 else (cg, wc)
        wy_out[role, 0:16, :] = jnp.concatenate(first[:2], axis=1)
        wy_out[role, 16:32, :] = jnp.concatenate([first[2], gate[:, half]], axis=1)
        rows = out_weight[:, half].astype(F32)
        wy_out[role, 32:40, :] = jnp.concatenate([rows[:8], rows[8:]], axis=1).astype(BF16)


def spread_kernel(tok, gain, edge, out):
    y = lax.axis_index("y")
    g = gain[...]
    high = g.astype(BF16)
    rest = g - high.astype(F32)
    middle = rest.astype(BF16)
    low = (rest - middle.astype(F32)).astype(BF16)
    row = lax.broadcasted_iota(jnp.int32, (8, LANES), 0)
    parts = [jnp.broadcast_to(part.astype(F32), (8, LANES)) for part in (high, middle, low)]
    gains = jnp.where(row == 0, parts[0], jnp.where(row == 1, parts[1], jnp.where(row == 2, parts[2], 0.0)))
    gains = gains.astype(BF16)
    block = tok[...]
    halo = jnp.where(y == YN - 1, edge[:WINDOW, :], edge[TOK - WINDOW :, :])
    for peer in range(PLANE):
        out[peer, :TOK, :] = block
        out[peer, TOK:SLOT, :] = halo
        out[peer, SLOT:, :] = gains


def mix_kernel(t, w, taps, sink, out, gate_0, gate_1, gate_2, gate_3, n_scr, p_scr, g_scr):
    y = lax.axis_index("y")
    z = lax.axis_index("z")
    gains = []
    for tp in range(TPN):
        r = t[tp, SLOT:, :].astype(F32)
        gains.append(r[0:1] + r[1:2] + r[2:3])
    segments = [(0, 0, TOK, WINDOW)]
    segments += [(WINDOW + TOK * b, b, 0, TOK) for b in range(YN)]
    segments += [(WINDOW + TOK * YN, YN - 1, TOK, WINDOW)]
    for at, b, start, count in segments:
        total = jnp.zeros((count, LANES), F32)
        for tp in range(TPN):
            x = t[b * TPN + tp, start : start + count, :].astype(F32)
            total = total + x * x
        scale = lax.rsqrt(jnp.sum(total, axis=1, keepdims=True) / FEATURES + EPSILON)
        for tp in range(TPN):
            x = t[b * TPN + tp, start : start + count, :].astype(F32)
            n_scr[at : at + count, LANES * tp : LANES * (tp + 1)] = (x * scale * gains[tp]).astype(BF16)
    weight = jnp.concatenate(
        [w[:, :, 16 * pair : 16 * pair + 16, :].reshape(FEATURES, LANES) for pair in range(2)], axis=1
    )
    p_scr[...] = nn_dot(n_scr[...], weight)
    left = lax.broadcasted_iota(jnp.int32, (TOK, LANES), 1) < HALF
    for b in range(YN):
        at = WINDOW + TOK * b
        g_scr[b] = jnp.where(left[:HALF], turned(p_scr[at : at + HALF, LANES:]), p_scr[at + HALF : at + TOK, LANES:])
    for k, gate in enumerate((gate_0, gate_1, gate_2, gate_3)):
        gate[...] = g_scr[lax.rem(y + k, YN)]

    def send(b, mixed):
        for tp in range(TPN):
            rows = w[2 * tp : 2 * tp + 2, :, 32:40, :].astype(F32).reshape(TPN, 8, LANES)
            rows = jnp.stack([turned(rows.reshape(HALF, LANES)).reshape(TPN, 8, LANES), rows], axis=1)
            out[b * TPN + tp] = jnp.where(left, mixed, rows.reshape(LANES, LANES).astype(BF16))

    @pl.when(y < 2)
    def _():
        logit = jnp.where(y == 0, sink[0], sink[1])
        span = TOK + 2 * WINDOW
        i = lax.broadcasted_iota(jnp.int32, (TOK, span), 0)
        j = lax.broadcasted_iota(jnp.int32, (TOK, span), 1)
        near = jnp.abs(i + WINDOW - j) <= WINDOW
        for b in range(YN):
            q = p_scr[WINDOW + TOK * b : WINDOW + TOK * (b + 1), :HALF].astype(BF16)
            k = p_scr[TOK * b : TOK * b + span, HALF:LANES].astype(BF16)
            v = p_scr[TOK * b : TOK * b + span, LANES:].astype(BF16)
            scores = nt_dot(q, k) * (HALF**-0.5)
            key = (z * YN + b) * TOK - WINDOW + j
            allowed = near & (key >= 0) & (key < ZN * YN * TOK)
            scores = jnp.where(allowed, scores, NEGATIVE)
            top = jnp.maximum(jnp.max(scores, axis=1, keepdims=True), logit)
            e = jnp.exp(scores - top)
            share = jnp.sum(e, axis=1, keepdims=True) + jnp.exp(logit - top)
            e = e / share
            high = e.astype(BF16)
            low = (e - high.astype(F32)).astype(BF16)
            send(b, (nn_dot(high, v) + nn_dot(low, v)).astype(BF16))

    @pl.when(y >= 2)
    def _():
        t3 = jnp.where(y == YN - 1, turned(taps[...]), taps[...])
        c = p_scr[:, :LANES].astype(BF16).astype(F32)
        p_scr[:, :LANES] = (c * turned(c)).astype(BF16).astype(F32)
        for b in range(YN):
            at = WINDOW + TOK * b
            before = p_scr[at - 1 : at - 1 + TOK, :LANES]
            here = p_scr[at : at + TOK, :LANES]
            after = p_scr[at + 1 : at + 1 + TOK, :LANES]
            post = p_scr[at : at + TOK, LANES:].astype(BF16).astype(F32)
            send(b, (post * (t3[0:1] * before + t3[1:2] * here + t3[2:3] * after)).astype(BF16))


def joined(a, b, left):
    return jnp.where(left, a, turned(b)), jnp.where(left, turned(a), b)


def gate_kernel(g_0, g_1, g_2, g_3, out, g_scr):
    y = lax.axis_index("y")
    for k, g in enumerate((g_0, g_1, g_2, g_3)):
        g_scr[k] = g[...]
    left = lax.broadcasted_iota(jnp.int32, (HALF, LANES), 1) < HALF
    for branch in range(2):
        parts = [g_scr[lax.rem(y + YN - source, YN)] for source in (2 * branch, 2 * branch + 1)]
        out[branch] = jax.nn.sigmoid(jnp.concatenate(joined(*parts, left), axis=0))


def final_kernel(m, gates, out):
    left = lax.broadcasted_iota(jnp.int32, (TOK, LANES), 1) < HALF
    total = jnp.zeros((TOK, LANES), F32)
    for branch in range(2):
        mixed, columns = [], []
        for tp in range(TPN):
            both = joined(m[(2 * branch) * TPN + tp], m[(2 * branch + 1) * TPN + tp], left)
            mixed.append(both[0])
            columns.append(both[1])
        value = nt_dot(jnp.concatenate(mixed, axis=1), jnp.concatenate(columns, axis=1))
        total = total + gates[branch] * value
    out[...] = total.astype(BF16)


VM = pl.BlockSpec(memory_space=pltpu.VMEM)
SM = pl.BlockSpec(memory_space=pltpu.SMEM)


def shaped(shape, kind=BF16):
    return jax.ShapeDtypeStruct(shape, kind)


def call(kernel, outs, args, specs=None, scratch=(), limit=8):
    return pl.pallas_call(
        kernel,
        out_shape=outs,
        in_specs=specs or [VM] * len(args),
        out_specs=jax.tree.map(lambda _: VM, outs),
        scratch_shapes=list(scratch),
        compiler_params=pltpu.CompilerParams(vmem_limit_bytes=limit * 2**20),
    )(*args)


def on_device(tok, gain, q, k, v, ci, pre, post, ag, cg, sink, taps, wa, wc):
    plane = ("y", "x", "c")
    edges = [(YN * z + YN - 1, YN * z + YN) for z in range(ZN - 1)]
    edge = lax.ppermute(tok, ("z", "y"), edges + [(b, a) for a, b in edges])
    wy = call(pack_kernel, shaped((YN, 40, LANES)), (q, k, v, ci, pre, post, ag, cg, wa.T, wc.T), limit=60)
    wy = lax.all_to_all(wy, "y", 0, 0, tiled=True)
    spread = call(spread_kernel, shaped((PLANE, SLOT + 8, LANES)), (tok, gain.reshape(1, LANES), edge), limit=60)
    gathered_tok = lax.all_to_all(spread, plane, 0, 0, tiled=True)
    w = lax.all_gather(wy.reshape(YN * 40, LANES), "z", axis=0, tiled=True).reshape(ZN, YN, 40, LANES)
    message, *gates = call(
        mix_kernel,
        (shaped((PLANE, TOK, LANES)),) + (shaped((HALF, LANES), F32),) * 4,
        (gathered_tok, w, taps, sink),
        [VM] * 3 + [SM],
        [
            pltpu.VMEM((ROWS, FEATURES), BF16),
            pltpu.VMEM((ROWS, 2 * LANES), F32),
            pltpu.VMEM((YN, HALF, LANES), F32),
        ],
        20,
    )
    message = lax.all_to_all(message, plane, 0, 0, tiled=True)
    for k in range(1, YN):
        gates[k] = lax.ppermute(gates[k], "y", [(y, (y + k) % YN) for y in range(YN)])
    gates = call(gate_kernel, shaped((2, TOK, LANES), F32), gates, scratch=[pltpu.VMEM((YN, HALF, LANES), F32)])
    return call(final_kernel, shaped((TOK, LANES)), (message, gates))


def solution(mesh):
    finer = Mesh(mesh.devices.reshape(ZN, YN, XN, CN), ("z", "y", "x", "c"))
    sp, tp = ("z", "y"), ("x", "c")
    rows = P(sp, tp)
    columns = P(tp, sp)
    return jax.shard_map(
        on_device,
        mesh=finer,
        in_specs=(rows, P(tp)) + (rows,) * 8 + (P(tp), P(None, tp), columns, columns),
        out_specs=rows,
        check_vma=False,
    )
```

```python
import jax
import jax.numpy as jnp
from jax import lax
from jax.experimental import pallas as pl
from jax.experimental.pallas import tpu as pltpu
from jax.sharding import Mesh
from jax.sharding import PartitionSpec as P


ZN, YN, XN, CN = 16, 4, 4, 2
TPN = XN * CN
PLANE = YN * TPN
HALF = 64
WINDOW = 64
LANES = 128
TOK = 128
ROWS = YN * TOK + 2 * WINDOW
SLOT = TOK + WINDOW
FEATURES = TPN * LANES
EPSILON = 1e-06
NEGATIVE = -1e30
F32 = jnp.float32
BF16 = jnp.bfloat16


def nt_dot(a, b):
    return lax.dot_general(a, b, (((1,), (1,)), ((), ())), preferred_element_type=F32)


def nn_dot(a, b):
    return jnp.dot(a, b, preferred_element_type=F32)


def turned(block):
    return jnp.concatenate([block[:, HALF:], block[:, :HALF]], axis=1)


def pack_kernel(q, k, v, ci, pre, post, ag, cg, wa, wc, wy_out):
    for role in range(YN):
        half = slice(HALF * (role % 2), HALF * (role % 2) + HALF)
        first = (q, k, v) if role < 2 else (ci, pre, post)
        first = [block[:, half] if block.shape[1] == LANES else block[...] for block in first]
        gate, out_weight = (cg if role % 2 else ag), (wa if role < 2 else wc)
        columns = first + [gate[:, :HALF], gate[:, HALF:], out_weight[:, half]]
        for pair in range(3):
            wy_out[role, 16 * pair : 16 * pair + 16, :] = jnp.concatenate(columns[2 * pair : 2 * pair + 2], axis=1)


def spread_kernel(tok, gain, edge, out):
    y = lax.axis_index("y")
    g = gain[...]
    high = g.astype(BF16)
    rest = g - high.astype(F32)
    middle = rest.astype(BF16)
    low = (rest - middle.astype(F32)).astype(BF16)
    row = lax.broadcasted_iota(jnp.int32, (8, LANES), 0)
    parts = [jnp.broadcast_to(part.astype(F32), (8, LANES)) for part in (high, middle, low)]
    gains = jnp.where(row == 0, parts[0], jnp.where(row == 1, parts[1], jnp.where(row == 2, parts[2], 0.0)))
    gains = gains.astype(BF16)
    block = tok[...]
    halo = jnp.where(y == YN - 1, edge[:WINDOW, :], edge[TOK - WINDOW :, :])
    for peer in range(PLANE):
        out[peer, :TOK, :] = block
        out[peer, TOK:SLOT, :] = halo
        out[peer, SLOT:, :] = gains


def mix_kernel(t, w, taps, sink, out, gate_own, gate_pair, n_scr, p_scr):
    y = lax.axis_index("y")
    z = lax.axis_index("z")
    gains = []
    for tp in range(TPN):
        r = t[tp, SLOT:, :].astype(F32)
        gains.append(r[0:1] + r[1:2] + r[2:3])
    segments = [(0, 0, TOK, WINDOW)]
    segments += [(WINDOW + TOK * b, b, 0, TOK) for b in range(YN)]
    segments += [(WINDOW + TOK * YN, YN - 1, TOK, WINDOW)]
    for at, b, start, count in segments:
        total = jnp.zeros((count, LANES), F32)
        for tp in range(TPN):
            x = t[b * TPN + tp, start : start + count, :].astype(F32)
            total = total + x * x
        scale = lax.rsqrt(jnp.sum(total, axis=1, keepdims=True) / FEATURES + EPSILON)
        for tp in range(TPN):
            x = t[b * TPN + tp, start : start + count, :].astype(F32)
            n_scr[at : at + count, LANES * tp : LANES * (tp + 1)] = (x * scale * gains[tp]).astype(BF16)
    blocks = [w[:, :, 16 * pair : 16 * pair + 16, :].reshape(FEATURES, LANES) for pair in range(3)]
    p_scr[...] = nn_dot(n_scr[...], jnp.concatenate(blocks[:2], axis=1))
    left = lax.broadcasted_iota(jnp.int32, (TOK, LANES), 1) < HALF
    for gate, owner in ((gate_own, y), (gate_pair, y + 1 - 2 * lax.rem(y, 2))):
        rows = pl.ds(pl.multiple_of(WINDOW + TOK * owner, WINDOW), TOK)
        gate[...] = turned(jnp.where(left, nn_dot(n_scr[rows, :], blocks[2]), p_scr[rows, LANES:]))

    def send(b, mixed):
        for tp in range(TPN):
            columns = w[2 * tp : 2 * tp + 2, :, 32:48, :].reshape(LANES, LANES)
            out[b * TPN + tp] = jnp.where(left, mixed, columns)

    @pl.when(y < 2)
    def _():
        logit = jnp.where(y == 0, sink[0], sink[1])
        span = TOK + 2 * WINDOW
        i = lax.broadcasted_iota(jnp.int32, (TOK, span), 0)
        j = lax.broadcasted_iota(jnp.int32, (TOK, span), 1)
        near = jnp.abs(i + WINDOW - j) <= WINDOW
        for b in range(YN):
            q = p_scr[WINDOW + TOK * b : WINDOW + TOK * (b + 1), :HALF].astype(BF16)
            k = p_scr[TOK * b : TOK * b + span, HALF:LANES].astype(BF16)
            v = p_scr[TOK * b : TOK * b + span, LANES:].astype(BF16)
            allowed = near
            if b == 0:
                allowed = near & (j >= jnp.where(z == 0, WINDOW, 0))
            if b == YN - 1:
                allowed = near & (j < jnp.where(z == ZN - 1, TOK + WINDOW, span))
            scores = jnp.where(allowed, nt_dot(q, k) * (HALF**-0.5), NEGATIVE)
            top = jnp.maximum(jnp.max(scores, axis=1, keepdims=True), logit)
            e = jnp.exp(scores - top)
            share = jnp.sum(e, axis=1, keepdims=True) + jnp.exp(logit - top)
            high = e.astype(BF16)
            low = (e - high.astype(F32)).astype(BF16)
            send(b, ((nn_dot(high, v) + nn_dot(low, v)) * (1.0 / share)).astype(BF16))

    @pl.when(y >= 2)
    def _():
        t3 = jnp.where(y == YN - 1, turned(taps[...]), taps[...])
        c = p_scr[:, :LANES].astype(BF16).astype(F32)
        p_scr[:, :LANES] = (c * turned(c)).astype(BF16).astype(F32)
        for b in range(YN):
            at = WINDOW + TOK * b
            before = p_scr[at - 1 : at - 1 + TOK, :LANES]
            here = p_scr[at : at + TOK, :LANES]
            after = p_scr[at + 1 : at + 1 + TOK, :LANES]
            post = p_scr[at : at + TOK, LANES:].astype(BF16).astype(F32)
            send(b, (post * (t3[0:1] * before + t3[1:2] * here + t3[2:3] * after)).astype(BF16))


def joined(a, b, left):
    return jnp.where(left, a, turned(b)), jnp.where(left, turned(a), b)


def gate_kernel(own, pair, out):
    even = lax.rem(lax.axis_index("y"), 2) == 0
    out[0] = jax.nn.sigmoid(jnp.where(even, own[...], pair[...]))
    out[1] = jax.nn.sigmoid(jnp.where(even, pair[...], own[...]))


def final_kernel(m, gates, out):
    left = lax.broadcasted_iota(jnp.int32, (TOK, LANES), 1) < HALF
    total = jnp.zeros((TOK, LANES), F32)
    for branch in range(2):
        mixed, columns = [], []
        for tp in range(TPN):
            both = joined(m[(2 * branch) * TPN + tp], m[(2 * branch + 1) * TPN + tp], left)
            mixed.append(both[0])
            columns.append(both[1])
        value = nt_dot(jnp.concatenate(mixed, axis=1), jnp.concatenate(columns, axis=1))
        total = total + gates[branch] * value
    out[...] = total.astype(BF16)


VM = pl.BlockSpec(memory_space=pltpu.VMEM)
SM = pl.BlockSpec(memory_space=pltpu.SMEM)


def shaped(shape, kind=BF16):
    return jax.ShapeDtypeStruct(shape, kind)


def call(kernel, outs, args, specs=None, scratch=(), limit=8):
    return pl.pallas_call(
        kernel,
        out_shape=outs,
        in_specs=specs or [VM] * len(args),
        out_specs=jax.tree.map(lambda _: VM, outs),
        scratch_shapes=list(scratch),
        compiler_params=pltpu.CompilerParams(vmem_limit_bytes=limit * 2**20),
    )(*args)


def on_device(tok, gain, q, k, v, ci, pre, post, ag, cg, sink, taps, wa, wc):
    plane = ("y", "x", "c")
    edges = [(YN * z + YN - 1, YN * z + YN) for z in range(ZN - 1)]
    wy = call(pack_kernel, shaped((YN, 48, LANES)), (q, k, v, ci, pre, post, ag, cg, wa.T, wc.T), limit=60)
    wy = lax.all_to_all(wy, "y", 0, 0, tiled=True)
    edge = lax.ppermute(tok, ("z", "y"), edges + [(b, a) for a, b in edges])
    spread = call(spread_kernel, shaped((PLANE, SLOT + 8, LANES)), (tok, gain.reshape(1, LANES), edge), limit=60)
    gathered_tok = lax.all_to_all(spread, plane, 0, 0, tiled=True)
    w = lax.all_gather(wy.reshape(YN * 48, LANES), "z", axis=0, tiled=True).reshape(ZN, YN, 48, LANES)
    message, own, pair = call(
        mix_kernel,
        (shaped((PLANE, TOK, LANES)),) + (shaped((TOK, LANES), F32),) * 2,
        (gathered_tok, w, taps, sink),
        [VM] * 3 + [SM],
        [pltpu.VMEM((ROWS, FEATURES), BF16), pltpu.VMEM((ROWS, 2 * LANES), F32)],
        20,
    )
    message = lax.all_to_all(message, plane, 0, 0, tiled=True)
    pair = lax.ppermute(pair, "y", [(y, y ^ 1) for y in range(YN)])
    gates = call(gate_kernel, shaped((2, TOK, LANES), F32), (own, pair))
    return call(final_kernel, shaped((TOK, LANES)), (message, gates))


def solution(mesh):
    finer = Mesh(mesh.devices.reshape(ZN, YN, XN, CN), ("z", "y", "x", "c"))
    sp, tp = ("z", "y"), ("x", "c")
    rows = P(sp, tp)
    columns = P(tp, sp)
    return jax.shard_map(
        on_device,
        mesh=finer,
        in_specs=(rows, P(tp)) + (rows,) * 8 + (P(tp), P(None, tp), columns, columns),
        out_specs=rows,
        check_vma=False,
    )
```

```python
import jax
import jax.numpy as jnp
from jax import lax
from jax.experimental import pallas as pl
from jax.experimental.pallas import tpu as pltpu
from jax.sharding import Mesh
from jax.sharding import PartitionSpec as P


ZN, YN, XN, CN = 16, 4, 4, 2
TPN = XN * CN
PLANE = YN * TPN
HALF = 64
WINDOW = 64
LANES = 128
TOK = 128
ROWS = YN * TOK + 2 * WINDOW
SLOT = TOK + WINDOW
FEATURES = TPN * LANES
EPSILON = 1e-06
NEGATIVE = -1e30
F32 = jnp.float32
BF16 = jnp.bfloat16


def nt_dot(a, b):
    return lax.dot_general(a, b, (((1,), (1,)), ((), ())), preferred_element_type=F32)


def nn_dot(a, b):
    return jnp.dot(a, b, preferred_element_type=F32)


def turned(block):
    return jnp.concatenate([block[:, HALF:], block[:, :HALF]], axis=1)


def pack_kernel(q, k, v, ci, pre, post, ag, cg, wa, wc, wy_out):
    for role in range(YN):
        half = slice(HALF * (role % 2), HALF * (role % 2) + HALF)
        first = (q, k, v) if role < 2 else (ci, pre, post)
        first = [block[:, half] if block.shape[1] == LANES else block[...] for block in first]
        gate, out_weight = (ag, wa) if role < 2 else (cg, wc)
        wy_out[role, 0:16, :] = jnp.concatenate(first[:2], axis=1)
        wy_out[role, 16:32, :] = jnp.concatenate([first[2], gate[:, half]], axis=1)
        rows = out_weight[:, half].astype(F32)
        wy_out[role, 32:40, :] = jnp.concatenate([rows[:8], rows[8:]], axis=1).astype(BF16)


def spread_kernel(tok, gain, edge, out):
    y = lax.axis_index("y")
    g = gain[...]
    high = g.astype(BF16)
    rest = g - high.astype(F32)
    middle = rest.astype(BF16)
    low = (rest - middle.astype(F32)).astype(BF16)
    row = lax.broadcasted_iota(jnp.int32, (8, LANES), 0)
    parts = [jnp.broadcast_to(part.astype(F32), (8, LANES)) for part in (high, middle, low)]
    gains = jnp.where(row == 0, parts[0], jnp.where(row == 1, parts[1], jnp.where(row == 2, parts[2], 0.0)))
    gains = gains.astype(BF16)
    block = tok[...]
    halo = jnp.where(y == YN - 1, edge[:WINDOW, :], edge[TOK - WINDOW :, :])
    for peer in range(PLANE):
        out[peer, :TOK, :] = block
        out[peer, TOK:SLOT, :] = halo
        out[peer, SLOT:, :] = gains


def mix_kernel(t, w, taps, sink, out, gate_0, gate_1, gate_2, gate_3, n_scr, p_scr, g_scr, w_scr, m_scr, sems):
    y = lax.axis_index("y")
    z = lax.axis_index("z")
    gains = []
    for tp in range(TPN):
        r = t[tp, SLOT:, :].astype(F32)
        gains.append(r[0:1] + r[1:2] + r[2:3])
    segments = [(0, 0, TOK, WINDOW)]
    segments += [(WINDOW + TOK * b, b, 0, TOK) for b in range(YN)]
    segments += [(WINDOW + TOK * YN, YN - 1, TOK, WINDOW)]
    for at, b, start, count in segments:
        total = jnp.zeros((count, LANES), F32)
        for tp in range(TPN):
            x = t[b * TPN + tp, start : start + count, :].astype(F32)
            total = total + x * x
        scale = lax.rsqrt(jnp.sum(total, axis=1, keepdims=True) / FEATURES + EPSILON)
        for tp in range(TPN):
            x = t[b * TPN + tp, start : start + count, :].astype(F32)
            n_scr[at : at + count, LANES * tp : LANES * (tp + 1)] = (x * scale * gains[tp]).astype(BF16)
    weight = jnp.concatenate(
        [w[:, :, 16 * pair : 16 * pair + 16, :].reshape(FEATURES, LANES) for pair in range(2)], axis=1
    )
    p_scr[...] = nn_dot(n_scr[...], weight)
    left = lax.broadcasted_iota(jnp.int32, (TOK, LANES), 1) < HALF
    for b in range(YN):
        at = WINDOW + TOK * b
        g_scr[b] = jnp.where(left[:HALF], turned(p_scr[at : at + HALF, LANES:]), p_scr[at + HALF : at + TOK, LANES:])
    for k, gate in enumerate((gate_0, gate_1, gate_2, gate_3)):
        gate[...] = g_scr[lax.rem(y + k, YN)]

    for tp in range(TPN):
        rows = w[2 * tp : 2 * tp + 2, :, 32:40, :].astype(F32).reshape(TPN, 8, LANES)
        rows = jnp.stack([turned(rows.reshape(HALF, LANES)).reshape(TPN, 8, LANES), rows], axis=1)
        w_scr[tp] = rows.reshape(LANES, LANES).astype(BF16)

    def outgoing(b):
        part = pl.ds(b * TPN, TPN)
        return pltpu.make_async_copy(m_scr.at[part], out.at[part], sems.at[b])

    def send(b, mixed):
        for tp in range(TPN):
            m_scr[b * TPN + tp] = jnp.where(left, mixed, w_scr[tp])
        outgoing(b).start()

    @pl.when(y < 2)
    def _():
        lane = lax.broadcasted_iota(jnp.int32, (1, 2), 1)
        logit = jnp.sum(jnp.where(lane == y, sink[...], 0.0), axis=1, keepdims=True)
        span = TOK + 2 * WINDOW
        i = lax.broadcasted_iota(jnp.int32, (TOK, span), 0)
        j = lax.broadcasted_iota(jnp.int32, (TOK, span), 1)
        near = jnp.abs(i + WINDOW - j) <= WINDOW
        for b in range(YN):
            q = p_scr[WINDOW + TOK * b : WINDOW + TOK * (b + 1), :HALF].astype(BF16)
            k = p_scr[TOK * b : TOK * b + span, HALF:LANES].astype(BF16)
            v = p_scr[TOK * b : TOK * b + span, LANES:].astype(BF16)
            scores = nt_dot(q, k) * (HALF**-0.5)
            allowed = near
            if b == 0:
                allowed = near & (j >= jnp.where(z == 0, WINDOW, 0))
            if b == YN - 1:
                allowed = near & (j < jnp.where(z == ZN - 1, TOK + WINDOW, span))
            scores = jnp.where(allowed, scores, NEGATIVE)
            top = jnp.maximum(jnp.max(scores, axis=1, keepdims=True), logit)
            e = jnp.exp(scores - top)
            share = jnp.sum(e, axis=1, keepdims=True) + jnp.exp(logit - top)
            high = e.astype(BF16)
            low = (e - high.astype(F32)).astype(BF16)
            send(b, ((nn_dot(high, v) + nn_dot(low, v)) * (1.0 / share)).astype(BF16))

    @pl.when(y >= 2)
    def _():
        t3 = jnp.where(y == YN - 1, turned(taps[...]), taps[...])
        c = p_scr[:, :LANES].astype(BF16).astype(F32)
        p_scr[:, :LANES] = (c * turned(c)).astype(BF16).astype(F32)
        for b in range(YN):
            at = WINDOW + TOK * b
            before = p_scr[at - 1 : at - 1 + TOK, :LANES]
            here = p_scr[at : at + TOK, :LANES]
            after = p_scr[at + 1 : at + 1 + TOK, :LANES]
            post = p_scr[at : at + TOK, LANES:].astype(BF16).astype(F32)
            send(b, (post * (t3[0:1] * before + t3[1:2] * here + t3[2:3] * after)).astype(BF16))

    for b in range(YN):
        outgoing(b).wait()


def joined(a, b, left):
    return jnp.where(left, a, turned(b)), jnp.where(left, turned(a), b)


def gate_kernel(g_0, g_1, g_2, g_3, out, g_scr):
    y = lax.axis_index("y")
    for k, g in enumerate((g_0, g_1, g_2, g_3)):
        g_scr[k] = g[...]
    left = lax.broadcasted_iota(jnp.int32, (HALF, LANES), 1) < HALF
    for branch in range(2):
        parts = [g_scr[lax.rem(y + YN - source, YN)] for source in (2 * branch, 2 * branch + 1)]
        out[branch] = jax.nn.sigmoid(jnp.concatenate(joined(*parts, left), axis=0))


def final_kernel(m, gates, out):
    left = lax.broadcasted_iota(jnp.int32, (TOK, LANES), 1) < HALF
    total = jnp.zeros((TOK, LANES), F32)
    for branch in range(2):
        mixed, columns = [], []
        for tp in range(TPN):
            both = joined(m[(2 * branch) * TPN + tp], m[(2 * branch + 1) * TPN + tp], left)
            mixed.append(both[0])
            columns.append(both[1])
        value = nt_dot(jnp.concatenate(mixed, axis=1), jnp.concatenate(columns, axis=1))
        total = total + gates[branch] * value
    out[...] = total.astype(BF16)


VM = pl.BlockSpec(memory_space=pltpu.VMEM)


def shaped(shape, kind=BF16):
    return jax.ShapeDtypeStruct(shape, kind)


def call(kernel, outs, args, specs=None, scratch=(), limit=8, first=None):
    out_specs = jax.tree.map(lambda _: VM, outs)
    if first is not None:
        out_specs = (first,) + out_specs[1:]
    return pl.pallas_call(
        kernel,
        out_shape=outs,
        in_specs=specs or [VM] * len(args),
        out_specs=out_specs,
        scratch_shapes=list(scratch),
        compiler_params=pltpu.CompilerParams(vmem_limit_bytes=limit * 2**20),
    )(*args)


def on_device(tok, gain, q, k, v, ci, pre, post, ag, cg, sink, taps, wa, wc):
    plane = ("y", "x", "c")
    edges = [(YN * z + YN - 1, YN * z + YN) for z in range(ZN - 1)]
    edge = lax.ppermute(tok, ("z", "y"), edges + [(b, a) for a, b in edges])
    wy = call(pack_kernel, shaped((YN, 40, LANES)), (q, k, v, ci, pre, post, ag, cg, wa.T, wc.T), limit=60)
    wy = lax.all_to_all(wy, "y", 0, 0, tiled=True)
    spread = call(spread_kernel, shaped((PLANE, SLOT + 8, LANES)), (tok, gain.reshape(1, LANES), edge), limit=60)
    gathered_tok = lax.all_to_all(spread, plane, 0, 0, tiled=True)
    w = lax.all_gather(wy.reshape(YN * 40, LANES), "z", axis=0, tiled=True).reshape(ZN, YN, 40, LANES)
    message, *gates = call(
        mix_kernel,
        (shaped((PLANE, TOK, LANES)),) + (shaped((HALF, LANES), F32),) * 4,
        (gathered_tok, w, taps, sink.reshape(1, 2)),
        [VM] * 4,
        [
            pltpu.VMEM((ROWS, FEATURES), BF16),
            pltpu.VMEM((ROWS, 2 * LANES), F32),
            pltpu.VMEM((YN, HALF, LANES), F32),
            pltpu.VMEM((TPN, LANES, LANES), BF16),
            pltpu.VMEM((PLANE, TOK, LANES), BF16),
            pltpu.SemaphoreType.DMA((YN,)),
        ],
        20,
        first=pl.BlockSpec(memory_space=pl.ANY),
    )
    message = lax.all_to_all(message, plane, 0, 0, tiled=True)
    for k in range(1, YN):
        gates[k] = lax.ppermute(gates[k], "y", [(y, (y + k) % YN) for y in range(YN)])
    gates = call(gate_kernel, shaped((2, TOK, LANES), F32), gates, scratch=[pltpu.VMEM((YN, HALF, LANES), F32)])
    return call(final_kernel, shaped((TOK, LANES)), (message, gates))


def solution(mesh):
    finer = Mesh(mesh.devices.reshape(ZN, YN, XN, CN), ("z", "y", "x", "c"))
    sp, tp = ("z", "y"), ("x", "c")
    rows = P(sp, tp)
    columns = P(tp, sp)
    return jax.shard_map(
        on_device,
        mesh=finer,
        in_specs=(rows, P(tp)) + (rows,) * 8 + (P(tp), P(None, tp), columns, columns),
        out_specs=rows,
        check_vma=False,
    )
```

```python
import jax
import jax.numpy as jnp
from jax import lax
from jax.experimental import pallas as pl
from jax.experimental.pallas import tpu as pltpu
from jax.sharding import Mesh
from jax.sharding import PartitionSpec as P


ZN, YN, XN, CN = 16, 4, 4, 2
TPN = XN * CN
PLANE = YN * TPN
HALF = 64
WINDOW = 64
LANES = 128
TOK = 128
ROWS = YN * TOK + 2 * WINDOW
SLOT = TOK + WINDOW
FEATURES = TPN * LANES
EPSILON = 1e-06
NEGATIVE = -1e30
F32 = jnp.float32
BF16 = jnp.bfloat16


def nt_dot(a, b):
    return lax.dot_general(a, b, (((1,), (1,)), ((), ())), preferred_element_type=F32)


def nn_dot(a, b):
    return jnp.dot(a, b, preferred_element_type=F32)


def turned(block):
    return jnp.concatenate([block[:, HALF:], block[:, :HALF]], axis=1)


def pack_kernel(q, k, v, ci, pre, post, ag, cg, wa, wc, wy_out):
    for role in range(YN):
        half = slice(HALF * (role % 2), HALF * (role % 2) + HALF)
        first = (q, k, v) if role < 2 else (ci, pre, post)
        first = [block[:, half] if block.shape[1] == LANES else block[...] for block in first]
        gate, out_weight = (cg if role % 2 else ag), (wa if role < 2 else wc)
        columns = first + [gate[:, :HALF], gate[:, HALF:], out_weight[:, half]]
        for pair in range(3):
            wy_out[role, 16 * pair : 16 * pair + 16, :] = jnp.concatenate(columns[2 * pair : 2 * pair + 2], axis=1)


def spread_kernel(tok, gain, edge, out):
    y = lax.axis_index("y")
    g = gain[...]
    high = g.astype(BF16)
    rest = g - high.astype(F32)
    middle = rest.astype(BF16)
    low = (rest - middle.astype(F32)).astype(BF16)
    row = lax.broadcasted_iota(jnp.int32, (8, LANES), 0)
    parts = [jnp.broadcast_to(part.astype(F32), (8, LANES)) for part in (high, middle, low)]
    gains = jnp.where(row == 0, parts[0], jnp.where(row == 1, parts[1], jnp.where(row == 2, parts[2], 0.0)))
    gains = gains.astype(BF16)
    block = tok[...]
    halo = jnp.where(y == YN - 1, edge[:WINDOW, :], edge[TOK - WINDOW :, :])
    for peer in range(PLANE):
        out[peer, :TOK, :] = block
        out[peer, TOK:SLOT, :] = halo
        out[peer, SLOT:, :] = gains


def mix_kernel(t, w, taps, sink, keep, give, gate_own, gate_pair, n_scr, p_scr, m_scr):
    y = lax.axis_index("y")
    z = lax.axis_index("z")
    gains = []
    for tp in range(TPN):
        r = t[tp, SLOT:, :].astype(F32)
        gains.append(r[0:1] + r[1:2] + r[2:3])
    segments = [(0, 0, TOK, WINDOW)]
    segments += [(WINDOW + TOK * b, b, 0, TOK) for b in range(YN)]
    segments += [(WINDOW + TOK * YN, YN - 1, TOK, WINDOW)]
    for at, b, start, count in segments:
        total = jnp.zeros((count, LANES), F32)
        for tp in range(TPN):
            x = t[b * TPN + tp, start : start + count, :].astype(F32)
            total = total + x * x
        scale = lax.rsqrt(jnp.sum(total, axis=1, keepdims=True) / FEATURES + EPSILON)
        for tp in range(TPN):
            x = t[b * TPN + tp, start : start + count, :].astype(F32)
            n_scr[at : at + count, LANES * tp : LANES * (tp + 1)] = (x * scale * gains[tp]).astype(BF16)
    blocks = [w[:, :, 16 * pair : 16 * pair + 16, :].reshape(FEATURES, LANES) for pair in range(3)]
    p_scr[...] = nn_dot(n_scr[...], jnp.concatenate(blocks[:2], axis=1))
    left = lax.broadcasted_iota(jnp.int32, (TOK, LANES), 1) < HALF
    for gate, owner in ((gate_own, y), (gate_pair, y + 1 - 2 * lax.rem(y, 2))):
        rows = pl.ds(pl.multiple_of(WINDOW + TOK * owner, WINDOW), TOK)
        gate[...] = turned(jnp.where(left, nn_dot(n_scr[rows, :], blocks[2]), p_scr[rows, LANES:]))

    def send(b, mixed):
        m_scr[TOK * b : TOK * (b + 1), :] = jnp.where(left, jnp.zeros_like(mixed), turned(mixed))

    @pl.when(y < 2)
    def _():
        lane = lax.broadcasted_iota(jnp.int32, (1, 2), 1)
        logit = jnp.sum(jnp.where(lane == y, sink[...], 0.0), axis=1, keepdims=True)
        span = TOK + 2 * WINDOW
        i = lax.broadcasted_iota(jnp.int32, (TOK, span), 0)
        j = lax.broadcasted_iota(jnp.int32, (TOK, span), 1)
        near = jnp.abs(i + WINDOW - j) <= WINDOW
        edge_low, edge_high = jnp.where(z == 0, WINDOW, 0), jnp.where(z == ZN - 1, TOK + WINDOW, span)
        masks = [near & (j >= edge_low)] + [near] * (YN - 2) + [near & (j < edge_high)]
        scores, tops, weights = [], [], []
        for b in range(YN):
            q = p_scr[WINDOW + TOK * b : WINDOW + TOK * (b + 1), :HALF].astype(BF16)
            k = p_scr[TOK * b : TOK * b + span, HALF:LANES].astype(BF16)
            scores.append(jnp.where(masks[b], nt_dot(q, k) * (HALF**-0.5), NEGATIVE))
        for b in range(YN):
            tops.append(jnp.maximum(jnp.max(scores[b], axis=1, keepdims=True), logit))
        for b in range(YN):
            weights.append(jnp.exp(scores[b] - tops[b]))
        for b in range(YN):
            v = p_scr[TOK * b : TOK * b + span, LANES:].astype(BF16)
            share = jnp.sum(weights[b], axis=1, keepdims=True) + jnp.exp(logit - tops[b])
            high = weights[b].astype(BF16)
            low = (weights[b] - high.astype(F32)).astype(BF16)
            send(b, ((nn_dot(high, v) + nn_dot(low, v)) * (1.0 / share)).astype(BF16))

    @pl.when(y >= 2)
    def _():
        t3 = jnp.where(y == YN - 1, turned(taps[...]), taps[...])
        c = p_scr[:, :LANES].astype(BF16).astype(F32)
        p_scr[:, :LANES] = (c * turned(c)).astype(BF16).astype(F32)
        for b in range(YN):
            at = WINDOW + TOK * b
            before = p_scr[at - 1 : at - 1 + TOK, :LANES]
            here = p_scr[at : at + TOK, :LANES]
            after = p_scr[at + 1 : at + 1 + TOK, :LANES]
            post = p_scr[at : at + TOK, LANES:].astype(BF16).astype(F32)
            send(b, (post * (t3[0:1] * before + t3[1:2] * here + t3[2:3] * after)).astype(BF16))

    first_core = lax.axis_index("c") == 0
    for b in range(YN):
        sums = nt_dot(m_scr[TOK * b : TOK * (b + 1), :], blocks[2])
        for x in range(XN):
            even = sums[:, 2 * LANES * x : 2 * LANES * x + LANES]
            odd = sums[:, 2 * LANES * x + LANES : 2 * LANES * (x + 1)]
            keep[XN * b + x] = jnp.where(first_core, even, odd)
            give[XN * b + x] = jnp.where(first_core, odd, even).astype(BF16)


def add_kernel(keep, came, out):
    out[...] = (keep[...] + came[...].astype(F32)).astype(BF16)


def gate_kernel(own, pair, out):
    even = lax.rem(lax.axis_index("y"), 2) == 0
    out[0] = jax.nn.sigmoid(jnp.where(even, own[...], pair[...]))
    out[1] = jax.nn.sigmoid(jnp.where(even, pair[...], own[...]))


def final_kernel(m, gates, out):
    total = jnp.zeros((TOK, LANES), F32)
    for branch in range(2):
        value = m[2 * XN * branch].astype(F32)
        for source in range(2 * XN * branch + 1, 2 * XN * (branch + 1)):
            value = value + m[source].astype(F32)
        total = total + gates[branch] * value
    out[...] = total.astype(BF16)


VM = pl.BlockSpec(memory_space=pltpu.VMEM)


def shaped(shape, kind=BF16):
    return jax.ShapeDtypeStruct(shape, kind)


def call(kernel, outs, args, specs=None, scratch=(), limit=8, first=None):
    out_specs = jax.tree.map(lambda _: VM, outs)
    if first is not None:
        out_specs = (first,) + out_specs[1:]
    return pl.pallas_call(
        kernel,
        out_shape=outs,
        in_specs=specs or [VM] * len(args),
        out_specs=out_specs,
        scratch_shapes=list(scratch),
        compiler_params=pltpu.CompilerParams(vmem_limit_bytes=limit * 2**20),
    )(*args)


def on_device(tok, gain, q, k, v, ci, pre, post, ag, cg, sink, taps, wa, wc):
    plane = ("y", "x", "c")
    edges = [(YN * z + YN - 1, YN * z + YN) for z in range(ZN - 1)]
    edge = lax.ppermute(tok, ("z", "y"), edges + [(b, a) for a, b in edges])
    wy = call(pack_kernel, shaped((YN, 48, LANES)), (q, k, v, ci, pre, post, ag, cg, wa.T, wc.T), limit=60)
    wy = lax.all_to_all(wy, "y", 0, 0, tiled=True)
    spread = call(spread_kernel, shaped((PLANE, SLOT + 8, LANES)), (tok, gain.reshape(1, LANES), edge), limit=60)
    gathered_tok = lax.all_to_all(spread, plane, 0, 0, tiled=True)
    w = lax.all_gather(wy.reshape(YN * 48, LANES), "z", axis=0, tiled=True).reshape(ZN, YN, 48, LANES)
    sums = (YN * XN, TOK, LANES)
    keep, give, own, pair = call(
        mix_kernel,
        (shaped(sums, F32), shaped(sums)) + (shaped((TOK, LANES), F32),) * 2,
        (gathered_tok, w, taps, sink.reshape(1, 2)),
        scratch=[
            pltpu.VMEM((ROWS, FEATURES), BF16),
            pltpu.VMEM((ROWS, 2 * LANES), F32),
            pltpu.VMEM((YN * TOK, LANES), BF16),
        ],
        limit=20,
    )
    came = lax.ppermute(give, "c", [(0, 1), (1, 0)])
    message = call(add_kernel, shaped(sums), (keep, came))
    message = lax.all_to_all(message, ("y", "x"), 0, 0, tiled=True)
    pair = lax.ppermute(pair, "y", [(y, y ^ 1) for y in range(YN)])
    gates = call(gate_kernel, shaped((2, TOK, LANES), F32), (own, pair))
    return call(final_kernel, shaped((TOK, LANES)), (message, gates))


def solution(mesh):
    finer = Mesh(mesh.devices.reshape(ZN, YN, XN, CN), ("z", "y", "x", "c"))
    sp, tp = ("z", "y"), ("x", "c")
    rows = P(sp, tp)
    columns = P(tp, sp)
    return jax.shard_map(
        on_device,
        mesh=finer,
        in_specs=(rows, P(tp)) + (rows,) * 8 + (P(tp), P(None, tp), columns, columns),
        out_specs=rows,
        check_vma=False,
    )
```

```python
import jax
import jax.numpy as jnp
from jax import lax
from jax.experimental import pallas as pl
from jax.experimental.pallas import tpu as pltpu
from jax.sharding import Mesh
from jax.sharding import PartitionSpec as P


ZN, YN, XN, CN = 16, 4, 4, 2
TPN = XN * CN
PLANE = YN * TPN
HALF = 64
WINDOW = 64
LANES = 128
TOK = 128
ROWS = YN * TOK + 2 * WINDOW
SLOT = TOK + WINDOW
FEATURES = TPN * LANES
EPSILON = 1e-06
NEGATIVE = -1e30
F32 = jnp.float32
BF16 = jnp.bfloat16


def nt_dot(a, b):
    return lax.dot_general(a, b, (((1,), (1,)), ((), ())), preferred_element_type=F32)


def nn_dot(a, b):
    return jnp.dot(a, b, preferred_element_type=F32)


def turned(block):
    return jnp.concatenate([block[:, HALF:], block[:, :HALF]], axis=1)


def pack_kernel(q, k, v, ci, pre, post, ag, cg, wa, wc, wy_out):
    for role in range(YN):
        half = slice(HALF * (role % 2), HALF * (role % 2) + HALF)
        first = (q, k, v) if role < 2 else (ci, pre, post)
        first = [block[:, half] if block.shape[1] == LANES else block[...] for block in first]
        gate, out_weight = (ag, wa) if role < 2 else (cg, wc)
        wy_out[role, 0:16, :] = jnp.concatenate(first[:2], axis=1)
        wy_out[role, 16:32, :] = jnp.concatenate([first[2], gate[:, half]], axis=1)
        rows = out_weight[:, half].astype(F32)
        wy_out[role, 32:40, :] = jnp.concatenate([rows[:8], rows[8:]], axis=1).astype(BF16)


def spread_kernel(tok, gain, edge, out):
    y = lax.axis_index("y")
    g = gain[...]
    high = g.astype(BF16)
    rest = g - high.astype(F32)
    middle = rest.astype(BF16)
    low = (rest - middle.astype(F32)).astype(BF16)
    row = lax.broadcasted_iota(jnp.int32, (8, LANES), 0)
    parts = [jnp.broadcast_to(part.astype(F32), (8, LANES)) for part in (high, middle, low)]
    gains = jnp.where(row == 0, parts[0], jnp.where(row == 1, parts[1], jnp.where(row == 2, parts[2], 0.0)))
    gains = gains.astype(BF16)
    block = tok[...]
    halo = jnp.where(y == YN - 1, edge[:WINDOW, :], edge[TOK - WINDOW :, :])
    for peer in range(PLANE):
        out[peer, :TOK, :] = block
        out[peer, TOK:SLOT, :] = halo
        out[peer, SLOT:, :] = gains


def mix_kernel(t, w, taps, sink, out, gate_0, gate_1, gate_2, gate_3, n_scr, p_scr, g_scr, w_scr, m_scr, sems):
    y = lax.axis_index("y")
    z = lax.axis_index("z")
    gains = []
    for tp in range(TPN):
        r = t[tp, SLOT:, :].astype(F32)
        gains.append(r[0:1] + r[1:2] + r[2:3])
    segments = [(0, 0, TOK, WINDOW)]
    segments += [(WINDOW + TOK * b, b, 0, TOK) for b in range(YN)]
    segments += [(WINDOW + TOK * YN, YN - 1, TOK, WINDOW)]
    for at, b, start, count in segments:
        total = jnp.zeros((count, LANES), F32)
        for tp in range(TPN):
            x = t[b * TPN + tp, start : start + count, :].astype(F32)
            total = total + x * x
        scale = lax.rsqrt(jnp.sum(total, axis=1, keepdims=True) / FEATURES + EPSILON)
        for tp in range(TPN):
            x = t[b * TPN + tp, start : start + count, :].astype(F32)
            n_scr[at : at + count, LANES * tp : LANES * (tp + 1)] = (x * scale * gains[tp]).astype(BF16)
    weight = jnp.concatenate(
        [w[:, :, 16 * pair : 16 * pair + 16, :].reshape(FEATURES, LANES) for pair in range(2)], axis=1
    )
    p_scr[...] = nn_dot(n_scr[...], weight)
    left = lax.broadcasted_iota(jnp.int32, (TOK, LANES), 1) < HALF
    for b in range(YN):
        at = WINDOW + TOK * b
        g_scr[b] = jnp.where(left[:HALF], turned(p_scr[at : at + HALF, LANES:]), p_scr[at + HALF : at + TOK, LANES:])
    for k, gate in enumerate((gate_0, gate_1, gate_2, gate_3)):
        gate[...] = g_scr[lax.rem(y + k, YN)]

    for tp in range(TPN):
        rows = w[2 * tp : 2 * tp + 2, :, 32:40, :].astype(F32).reshape(TPN, 8, LANES)
        rows = jnp.stack([turned(rows.reshape(HALF, LANES)).reshape(TPN, 8, LANES), rows], axis=1)
        w_scr[tp] = rows.reshape(LANES, LANES).astype(BF16)

    def outgoing(b):
        part = pl.ds(b * TPN, TPN)
        return pltpu.make_async_copy(m_scr.at[part], out.at[part], sems.at[b])

    def send(b, mixed):
        for tp in range(TPN):
            m_scr[b * TPN + tp] = jnp.where(left, mixed, w_scr[tp])
        outgoing(b).start()

    @pl.when(y < 2)
    def _():
        lane = lax.broadcasted_iota(jnp.int32, (1, 2), 1)
        logit = jnp.sum(jnp.where(lane == y, sink[...], 0.0), axis=1, keepdims=True)
        span = TOK + 2 * WINDOW
        i = lax.broadcasted_iota(jnp.int32, (TOK, span), 0)
        j = lax.broadcasted_iota(jnp.int32, (TOK, span), 1)
        near = jnp.abs(i + WINDOW - j) <= WINDOW
        edge_low, edge_high = jnp.where(z == 0, WINDOW, 0), jnp.where(z == ZN - 1, TOK + WINDOW, span)
        masks = [near & (j >= edge_low)] + [near] * (YN - 2) + [near & (j < edge_high)]
        scores, tops, weights = [], [], []
        for b in range(YN):
            q = p_scr[WINDOW + TOK * b : WINDOW + TOK * (b + 1), :HALF].astype(BF16)
            k = p_scr[TOK * b : TOK * b + span, HALF:LANES].astype(BF16)
            scores.append(jnp.where(masks[b], nt_dot(q, k) * (HALF**-0.5), NEGATIVE))
        for b in range(YN):
            tops.append(jnp.maximum(jnp.max(scores[b], axis=1, keepdims=True), logit))
        for b in range(YN):
            weights.append(jnp.exp(scores[b] - tops[b]))
        for b in range(YN):
            v = p_scr[TOK * b : TOK * b + span, LANES:].astype(BF16)
            share = jnp.sum(weights[b], axis=1, keepdims=True) + jnp.exp(logit - tops[b])
            high = weights[b].astype(BF16)
            low = (weights[b] - high.astype(F32)).astype(BF16)
            send(b, ((nn_dot(high, v) + nn_dot(low, v)) * (1.0 / share)).astype(BF16))

    @pl.when(y >= 2)
    def _():
        t3 = jnp.where(y == YN - 1, turned(taps[...]), taps[...])
        c = p_scr[:, :LANES].astype(BF16).astype(F32)
        p_scr[:, :LANES] = (c * turned(c)).astype(BF16).astype(F32)
        for b in range(YN):
            at = WINDOW + TOK * b
            before = p_scr[at - 1 : at - 1 + TOK, :LANES]
            here = p_scr[at : at + TOK, :LANES]
            after = p_scr[at + 1 : at + 1 + TOK, :LANES]
            post = p_scr[at : at + TOK, LANES:].astype(BF16).astype(F32)
            send(b, (post * (t3[0:1] * before + t3[1:2] * here + t3[2:3] * after)).astype(BF16))

    for b in range(YN):
        outgoing(b).wait()


def joined(a, b, left):
    return jnp.where(left, a, turned(b)), jnp.where(left, turned(a), b)


def gate_kernel(g_0, g_1, g_2, g_3, out, g_scr):
    y = lax.axis_index("y")
    for k, g in enumerate((g_0, g_1, g_2, g_3)):
        g_scr[k] = g[...]
    left = lax.broadcasted_iota(jnp.int32, (HALF, LANES), 1) < HALF
    for branch in range(2):
        parts = [g_scr[lax.rem(y + YN - source, YN)] for source in (2 * branch, 2 * branch + 1)]
        out[branch] = jax.nn.sigmoid(jnp.concatenate(joined(*parts, left), axis=0))


def final_kernel(m, gates, out):
    left = lax.broadcasted_iota(jnp.int32, (TOK, LANES), 1) < HALF
    total = jnp.zeros((TOK, LANES), F32)
    for branch in range(2):
        mixed, columns = [], []
        for tp in range(TPN):
            both = joined(m[(2 * branch) * TPN + tp], m[(2 * branch + 1) * TPN + tp], left)
            mixed.append(both[0])
            columns.append(both[1])
        value = nt_dot(jnp.concatenate(mixed, axis=1), jnp.concatenate(columns, axis=1))
        total = total + gates[branch] * value
    out[...] = total.astype(BF16)


VM = pl.BlockSpec(memory_space=pltpu.VMEM)


def shaped(shape, kind=BF16):
    return jax.ShapeDtypeStruct(shape, kind)


def call(kernel, outs, args, specs=None, scratch=(), limit=8, first=None):
    out_specs = jax.tree.map(lambda _: VM, outs)
    if first is not None:
        out_specs = (first,) + out_specs[1:]
    return pl.pallas_call(
        kernel,
        out_shape=outs,
        in_specs=specs or [VM] * len(args),
        out_specs=out_specs,
        scratch_shapes=list(scratch),
        compiler_params=pltpu.CompilerParams(vmem_limit_bytes=limit * 2**20),
    )(*args)


def on_device(tok, gain, q, k, v, ci, pre, post, ag, cg, sink, taps, wa, wc):
    plane = ("y", "x", "c")
    edges = [(YN * z + YN - 1, YN * z + YN) for z in range(ZN - 1)]
    edge = lax.ppermute(tok, ("z", "y"), edges + [(b, a) for a, b in edges])
    wy = call(pack_kernel, shaped((YN, 40, LANES)), (q, k, v, ci, pre, post, ag, cg, wa.T, wc.T), limit=60)
    wy = lax.all_to_all(wy, "y", 0, 0, tiled=True)
    spread = call(spread_kernel, shaped((PLANE, SLOT + 8, LANES)), (tok, gain.reshape(1, LANES), edge), limit=60)
    gathered_tok = lax.all_to_all(spread, plane, 0, 0, tiled=True)
    w = lax.all_gather(wy.reshape(YN * 40, LANES), "z", axis=0, tiled=True).reshape(ZN, YN, 40, LANES)
    message, *gates = call(
        mix_kernel,
        (shaped((PLANE, TOK, LANES)),) + (shaped((HALF, LANES), F32),) * 4,
        (gathered_tok, w, taps, sink.reshape(1, 2)),
        [VM] * 4,
        [
            pltpu.VMEM((ROWS, FEATURES), BF16),
            pltpu.VMEM((ROWS, 2 * LANES), F32),
            pltpu.VMEM((YN, HALF, LANES), F32),
            pltpu.VMEM((TPN, LANES, LANES), BF16),
            pltpu.VMEM((PLANE, TOK, LANES), BF16),
            pltpu.SemaphoreType.DMA((YN,)),
        ],
        20,
        first=pl.BlockSpec(memory_space=pl.ANY),
    )
    message = lax.all_to_all(message, plane, 0, 0, tiled=True)
    for k in range(1, YN):
        gates[k] = lax.ppermute(gates[k], "y", [(y, (y + k) % YN) for y in range(YN)])
    gates = call(gate_kernel, shaped((2, TOK, LANES), F32), gates, scratch=[pltpu.VMEM((YN, HALF, LANES), F32)])
    return call(final_kernel, shaped((TOK, LANES)), (message, gates))


def solution(mesh):
    finer = Mesh(mesh.devices.reshape(ZN, YN, XN, CN), ("z", "y", "x", "c"))
    sp, tp = ("z", "y"), ("x", "c")
    rows = P(sp, tp)
    columns = P(tp, sp)
    return jax.shard_map(
        on_device,
        mesh=finer,
        in_specs=(rows, P(tp)) + (rows,) * 8 + (P(tp), P(None, tp), columns, columns),
        out_specs=rows,
        check_vma=False,
    )
```

```python
import jax
import jax.numpy as jnp
from jax import lax
from jax.experimental import pallas as pl
from jax.experimental.pallas import tpu as pltpu
from jax.sharding import Mesh
from jax.sharding import PartitionSpec as P


ZN, YN, XN, CN = 16, 4, 4, 2
TPN = XN * CN
PLANE = YN * TPN
HALF = 64
WINDOW = 64
LANES = 128
TOK = 128
ROWS = YN * TOK + 2 * WINDOW
SLOT = TOK + WINDOW
FEATURES = TPN * LANES
EPSILON = 1e-06
NEGATIVE = -1e30
F32 = jnp.float32
BF16 = jnp.bfloat16


def nt_dot(a, b):
    return lax.dot_general(a, b, (((1,), (1,)), ((), ())), preferred_element_type=F32)


def nn_dot(a, b):
    return jnp.dot(a, b, preferred_element_type=F32)


def turned(block):
    return jnp.concatenate([block[:, HALF:], block[:, :HALF]], axis=1)


def pack_kernel(q, k, v, ci, pre, post, ag, cg, wa, wc, wy_out):
    for role in range(YN):
        half = slice(HALF * (role % 2), HALF * (role % 2) + HALF)
        first = (q, k, v) if role < 2 else (ci, pre, post)
        first = [block[:, half] if block.shape[1] == LANES else block[...] for block in first]
        gate, out_weight = (ag, wa) if role < 2 else (cg, wc)
        wy_out[role, 0:16, :] = jnp.concatenate(first[:2], axis=1)
        wy_out[role, 16:32, :] = jnp.concatenate([first[2], gate[:, half]], axis=1)
        rows = out_weight[:, half].astype(F32)
        wy_out[role, 32:40, :] = jnp.concatenate([rows[:8], rows[8:]], axis=1).astype(BF16)


def spread_kernel(tok, gain, edge, out):
    y = lax.axis_index("y")
    g = gain[...]
    high = g.astype(BF16)
    rest = g - high.astype(F32)
    middle = rest.astype(BF16)
    low = (rest - middle.astype(F32)).astype(BF16)
    row = lax.broadcasted_iota(jnp.int32, (8, LANES), 0)
    parts = [jnp.broadcast_to(part.astype(F32), (8, LANES)) for part in (high, middle, low)]
    gains = jnp.where(row == 0, parts[0], jnp.where(row == 1, parts[1], jnp.where(row == 2, parts[2], 0.0)))
    gains = gains.astype(BF16)
    block = tok[...]
    halo = jnp.where(y == YN - 1, edge[:WINDOW, :], edge[TOK - WINDOW :, :])
    for peer in range(PLANE):
        out[peer, :TOK, :] = block
        out[peer, TOK:SLOT, :] = halo
        out[peer, SLOT:, :] = gains


def mix_kernel(t, w, taps, sink, out, gate_0, gate_1, gate_2, gate_3, n_scr, p_scr, g_scr, w_scr, m_scr, sems):
    y = lax.axis_index("y")
    z = lax.axis_index("z")
    gains = []
    for tp in range(TPN):
        r = t[YN * tp, SLOT:, :].astype(F32)
        gains.append(r[0:1] + r[1:2] + r[2:3])
    segments = [(0, 0, TOK, WINDOW)]
    segments += [(WINDOW + TOK * b, b, 0, TOK) for b in range(YN)]
    segments += [(WINDOW + TOK * YN, YN - 1, TOK, WINDOW)]
    for at, b, start, count in segments:
        total = jnp.zeros((count, LANES), F32)
        for tp in range(TPN):
            x = t[YN * tp + b, start : start + count, :].astype(F32)
            total = total + x * x
        scale = lax.rsqrt(jnp.sum(total, axis=1, keepdims=True) / FEATURES + EPSILON)
        for tp in range(TPN):
            x = t[YN * tp + b, start : start + count, :].astype(F32)
            n_scr[at : at + count, LANES * tp : LANES * (tp + 1)] = (x * scale * gains[tp]).astype(BF16)
    weight = jnp.concatenate(
        [w[:, :, 16 * pair : 16 * pair + 16, :].reshape(FEATURES, LANES) for pair in range(2)], axis=1
    )
    p_scr[...] = nn_dot(n_scr[...], weight)
    left = lax.broadcasted_iota(jnp.int32, (TOK, LANES), 1) < HALF
    for b in range(YN):
        at = WINDOW + TOK * b
        g_scr[b] = jnp.where(left[:HALF], turned(p_scr[at : at + HALF, LANES:]), p_scr[at + HALF : at + TOK, LANES:])
    for k, gate in enumerate((gate_0, gate_1, gate_2, gate_3)):
        gate[...] = g_scr[lax.rem(y + k, YN)]

    for tp in range(TPN):
        rows = w[2 * tp : 2 * tp + 2, :, 32:40, :].astype(F32).reshape(TPN, 8, LANES)
        rows = jnp.stack([turned(rows.reshape(HALF, LANES)).reshape(TPN, 8, LANES), rows], axis=1)
        w_scr[tp] = rows.reshape(LANES, LANES).astype(BF16)

    def outgoing(b):
        return pltpu.make_async_copy(m_scr.at[:, b], out.at[:, b], sems.at[b])

    def send(b, mixed):
        for tp in range(TPN):
            m_scr[tp, b] = jnp.where(left, mixed, w_scr[tp])
        outgoing(b).start()

    @pl.when(y < 2)
    def _():
        lane = lax.broadcasted_iota(jnp.int32, (1, 2), 1)
        logit = jnp.sum(jnp.where(lane == y, sink[...], 0.0), axis=1, keepdims=True)
        span = TOK + 2 * WINDOW
        i = lax.broadcasted_iota(jnp.int32, (TOK, span), 0)
        j = lax.broadcasted_iota(jnp.int32, (TOK, span), 1)
        near = jnp.abs(i + WINDOW - j) <= WINDOW
        edge_low, edge_high = jnp.where(z == 0, WINDOW, 0), jnp.where(z == ZN - 1, TOK + WINDOW, span)
        masks = [near & (j >= edge_low)] + [near] * (YN - 2) + [near & (j < edge_high)]
        scores, tops, weights = [], [], []
        for b in range(YN):
            q = p_scr[WINDOW + TOK * b : WINDOW + TOK * (b + 1), :HALF].astype(BF16)
            k = p_scr[TOK * b : TOK * b + span, HALF:LANES].astype(BF16)
            scores.append(jnp.where(masks[b], nt_dot(q, k) * (HALF**-0.5), NEGATIVE))
        for b in range(YN):
            tops.append(jnp.maximum(jnp.max(scores[b], axis=1, keepdims=True), logit))
        for b in range(YN):
            weights.append(jnp.exp(scores[b] - tops[b]))
        for b in range(YN):
            v = p_scr[TOK * b : TOK * b + span, LANES:].astype(BF16)
            share = jnp.sum(weights[b], axis=1, keepdims=True) + jnp.exp(logit - tops[b])
            high = weights[b].astype(BF16)
            low = (weights[b] - high.astype(F32)).astype(BF16)
            send(b, ((nn_dot(high, v) + nn_dot(low, v)) * (1.0 / share)).astype(BF16))

    @pl.when(y >= 2)
    def _():
        t3 = jnp.where(y == YN - 1, turned(taps[...]), taps[...])
        c = p_scr[:, :LANES].astype(BF16).astype(F32)
        p_scr[:, :LANES] = (c * turned(c)).astype(BF16).astype(F32)
        for b in range(YN):
            at = WINDOW + TOK * b
            before = p_scr[at - 1 : at - 1 + TOK, :LANES]
            here = p_scr[at : at + TOK, :LANES]
            after = p_scr[at + 1 : at + 1 + TOK, :LANES]
            post = p_scr[at : at + TOK, LANES:].astype(BF16).astype(F32)
            send(b, (post * (t3[0:1] * before + t3[1:2] * here + t3[2:3] * after)).astype(BF16))

    for b in range(YN):
        outgoing(b).wait()


def joined(a, b, left):
    return jnp.where(left, a, turned(b)), jnp.where(left, turned(a), b)


def gate_kernel(g_0, g_1, g_2, g_3, out, g_scr):
    y = lax.axis_index("y")
    for k, g in enumerate((g_0, g_1, g_2, g_3)):
        g_scr[k] = g[...]
    left = lax.broadcasted_iota(jnp.int32, (HALF, LANES), 1) < HALF
    for branch in range(2):
        parts = [g_scr[lax.rem(y + YN - source, YN)] for source in (2 * branch, 2 * branch + 1)]
        out[branch] = jax.nn.sigmoid(jnp.concatenate(joined(*parts, left), axis=0))


def final_kernel(m, gates, out):
    left = lax.broadcasted_iota(jnp.int32, (TOK, LANES), 1) < HALF
    total = jnp.zeros((TOK, LANES), F32)
    for branch in range(2):
        mixed, columns = [], []
        for tp in range(TPN):
            both = joined(m[YN * tp + 2 * branch], m[YN * tp + 2 * branch + 1], left)
            mixed.append(both[0])
            columns.append(both[1])
        value = nt_dot(jnp.concatenate(mixed, axis=1), jnp.concatenate(columns, axis=1))
        total = total + gates[branch] * value
    out[...] = total.astype(BF16)


VM = pl.BlockSpec(memory_space=pltpu.VMEM)


def shaped(shape, kind=BF16):
    return jax.ShapeDtypeStruct(shape, kind)


def call(kernel, outs, args, specs=None, scratch=(), limit=8, first=None):
    out_specs = jax.tree.map(lambda _: VM, outs)
    if first is not None:
        out_specs = (first,) + out_specs[1:]
    return pl.pallas_call(
        kernel,
        out_shape=outs,
        in_specs=specs or [VM] * len(args),
        out_specs=out_specs,
        scratch_shapes=list(scratch),
        compiler_params=pltpu.CompilerParams(vmem_limit_bytes=limit * 2**20),
    )(*args)


def on_device(tok, gain, q, k, v, ci, pre, post, ag, cg, sink, taps, wa, wc):
    plane = ("x", "c", "y")
    edges = [(YN * z + YN - 1, YN * z + YN) for z in range(ZN - 1)]
    edge = lax.ppermute(tok, ("z", "y"), edges + [(b, a) for a, b in edges])
    wy = call(pack_kernel, shaped((YN, 40, LANES)), (q, k, v, ci, pre, post, ag, cg, wa.T, wc.T), limit=60)
    wy = lax.all_to_all(wy, "y", 0, 0, tiled=True)
    spread = call(spread_kernel, shaped((PLANE, SLOT + 8, LANES)), (tok, gain.reshape(1, LANES), edge), limit=60)
    gathered_tok = lax.all_to_all(spread, plane, 0, 0, tiled=True)
    w = lax.all_gather(wy.reshape(YN * 40, LANES), "z", axis=0, tiled=True).reshape(ZN, YN, 40, LANES)
    message, *gates = call(
        mix_kernel,
        (shaped((TPN, YN, TOK, LANES)),) + (shaped((HALF, LANES), F32),) * 4,
        (gathered_tok, w, taps, sink.reshape(1, 2)),
        [VM] * 4,
        [
            pltpu.VMEM((ROWS, FEATURES), BF16),
            pltpu.VMEM((ROWS, 2 * LANES), F32),
            pltpu.VMEM((YN, HALF, LANES), F32),
            pltpu.VMEM((TPN, LANES, LANES), BF16),
            pltpu.VMEM((TPN, YN, TOK, LANES), BF16),
            pltpu.SemaphoreType.DMA((YN,)),
        ],
        20,
        first=pl.BlockSpec(memory_space=pl.ANY),
    )
    message = lax.all_to_all(message.reshape(PLANE, TOK, LANES), plane, 0, 0, tiled=True)
    for k in range(1, YN):
        gates[k] = lax.ppermute(gates[k], "y", [(y, (y + k) % YN) for y in range(YN)])
    gates = call(gate_kernel, shaped((2, TOK, LANES), F32), gates, scratch=[pltpu.VMEM((YN, HALF, LANES), F32)])
    return call(final_kernel, shaped((TOK, LANES)), (message, gates))


def solution(mesh):
    finer = Mesh(mesh.devices.reshape(ZN, YN, XN, CN), ("z", "y", "x", "c"))
    sp, tp = ("z", "y"), ("x", "c")
    rows = P(sp, tp)
    columns = P(tp, sp)
    return jax.shard_map(
        on_device,
        mesh=finer,
        in_specs=(rows, P(tp)) + (rows,) * 8 + (P(tp), P(None, tp), columns, columns),
        out_specs=rows,
        check_vma=False,
    )
```

```python
import jax
import jax.numpy as jnp
from jax import lax
from jax.experimental import pallas as pl
from jax.experimental.pallas import tpu as pltpu
from jax.sharding import Mesh
from jax.sharding import PartitionSpec as P


ZN, YN, XN, CN = 16, 4, 4, 2
TPN = XN * CN
PLANE = YN * TPN
HALF = 64
WINDOW = 64
LANES = 128
TOK = 128
ROWS = YN * TOK + 2 * WINDOW
SLOT = TOK + WINDOW
FEATURES = TPN * LANES
EPSILON = 1e-06
NEGATIVE = -1e30
F32 = jnp.float32
BF16 = jnp.bfloat16


def nt_dot(a, b):
    return lax.dot_general(a, b, (((1,), (1,)), ((), ())), preferred_element_type=F32)


def nn_dot(a, b):
    return jnp.dot(a, b, preferred_element_type=F32)


def turned(block):
    return jnp.concatenate([block[:, HALF:], block[:, :HALF]], axis=1)


def pack_kernel(q, k, v, ci, pre, post, ag, cg, wa, wc, wy_out):
    for role in range(YN):
        half = slice(HALF * (role % 2), HALF * (role % 2) + HALF)
        first = (q, k, v) if role < 2 else (ci, pre, post)
        first = [block[:, half] if block.shape[1] == LANES else block[...] for block in first]
        gate, out_weight = (ag, wa) if role < 2 else (cg, wc)
        wy_out[role, 0:16, :] = jnp.concatenate(first[:2], axis=1)
        wy_out[role, 16:32, :] = jnp.concatenate([first[2], gate[:, half]], axis=1)
        rows = out_weight[:, half].astype(F32)
        wy_out[role, 32:40, :] = jnp.concatenate([rows[:8], rows[8:]], axis=1).astype(BF16)


def spread_kernel(tok, gain, edge, out):
    y = lax.axis_index("y")
    g = gain[...]
    high = g.astype(BF16)
    rest = g - high.astype(F32)
    middle = rest.astype(BF16)
    low = (rest - middle.astype(F32)).astype(BF16)
    row = lax.broadcasted_iota(jnp.int32, (8, LANES), 0)
    parts = [jnp.broadcast_to(part.astype(F32), (8, LANES)) for part in (high, middle, low)]
    gains = jnp.where(row == 0, parts[0], jnp.where(row == 1, parts[1], jnp.where(row == 2, parts[2], 0.0)))
    gains = gains.astype(BF16)
    block = tok[...]
    halo = jnp.where(y == YN - 1, edge[:WINDOW, :], edge[TOK - WINDOW :, :])
    for peer in range(PLANE):
        out[peer, :TOK, :] = block
        out[peer, TOK:SLOT, :] = halo
        out[peer, SLOT:, :] = gains


def mix_kernel(t, w, taps, sink, out, gate_0, gate_1, gate_2, gate_3, n_scr, p_scr, g_scr, w_scr, m_scr, sems):
    y = lax.axis_index("y")
    z = lax.axis_index("z")
    gains = []
    for tp in range(TPN):
        r = t[YN * tp, SLOT:, :].astype(F32)
        gains.append(r[0:1] + r[1:2] + r[2:3])
    segments = [(0, 0, TOK, WINDOW)]
    segments += [(WINDOW + TOK * b, b, 0, TOK) for b in range(YN)]
    segments += [(WINDOW + TOK * YN, YN - 1, TOK, WINDOW)]
    for at, b, start, count in segments:
        total = jnp.zeros((count, LANES), F32)
        for tp in range(TPN):
            x = t[YN * tp + b, start : start + count, :].astype(F32)
            total = total + x * x
        scale = lax.rsqrt(jnp.sum(total, axis=1, keepdims=True) / FEATURES + EPSILON)
        for tp in range(TPN):
            x = t[YN * tp + b, start : start + count, :].astype(F32)
            n_scr[at : at + count, LANES * tp : LANES * (tp + 1)] = (x * scale * gains[tp]).astype(BF16)
    weight = jnp.concatenate(
        [w[:, :, 16 * pair : 16 * pair + 16, :].reshape(FEATURES, LANES) for pair in range(2)], axis=1
    )
    p_scr[...] = nn_dot(n_scr[...], weight)
    left = lax.broadcasted_iota(jnp.int32, (TOK, LANES), 1) < HALF
    for b in range(YN):
        at = WINDOW + TOK * b
        g_scr[b] = jnp.where(left[:HALF], turned(p_scr[at : at + HALF, LANES:]), p_scr[at + HALF : at + TOK, LANES:])
    for k, gate in enumerate((gate_0, gate_1, gate_2, gate_3)):
        gate[...] = g_scr[lax.rem(y + k, YN)]

    for tp in range(TPN):
        rows = w[2 * tp : 2 * tp + 2, :, 32:40, :].astype(F32).reshape(TPN, 8, LANES)
        rows = jnp.stack([turned(rows.reshape(HALF, LANES)).reshape(TPN, 8, LANES), rows], axis=1)
        w_scr[tp] = rows.reshape(LANES, LANES).astype(BF16)

    for x in range(XN):
        packed = jnp.where(left[:HALF], turned(w_scr[2 * x + 1])[:HALF], w_scr[2 * x + 1][HALF:])
        for b in range(YN):
            m_scr[x, b, TOK:, :] = packed

    def outgoing(b):
        return pltpu.make_async_copy(m_scr.at[:, b], out.at[:, b], sems.at[b])

    def send(b, mixed):
        for x in range(XN):
            m_scr[x, b, :TOK, :] = jnp.where(left, mixed, w_scr[2 * x])
        outgoing(b).start()

    @pl.when(y < 2)
    def _():
        lane = lax.broadcasted_iota(jnp.int32, (1, 2), 1)
        logit = jnp.sum(jnp.where(lane == y, sink[...], 0.0), axis=1, keepdims=True)
        span = TOK + 2 * WINDOW
        i = lax.broadcasted_iota(jnp.int32, (TOK, span), 0)
        j = lax.broadcasted_iota(jnp.int32, (TOK, span), 1)
        near = jnp.abs(i + WINDOW - j) <= WINDOW
        edge_low, edge_high = jnp.where(z == 0, WINDOW, 0), jnp.where(z == ZN - 1, TOK + WINDOW, span)
        masks = [near & (j >= edge_low)] + [near] * (YN - 2) + [near & (j < edge_high)]
        scores, tops, weights = [], [], []
        for b in range(YN):
            q = p_scr[WINDOW + TOK * b : WINDOW + TOK * (b + 1), :HALF].astype(BF16)
            k = p_scr[TOK * b : TOK * b + span, HALF:LANES].astype(BF16)
            scores.append(jnp.where(masks[b], nt_dot(q, k) * (HALF**-0.5), NEGATIVE))
        for b in range(YN):
            tops.append(jnp.maximum(jnp.max(scores[b], axis=1, keepdims=True), logit))
        for b in range(YN):
            weights.append(jnp.exp(scores[b] - tops[b]))
        for b in range(YN):
            v = p_scr[TOK * b : TOK * b + span, LANES:].astype(BF16)
            share = jnp.sum(weights[b], axis=1, keepdims=True) + jnp.exp(logit - tops[b])
            high = weights[b].astype(BF16)
            low = (weights[b] - high.astype(F32)).astype(BF16)
            send(b, ((nn_dot(high, v) + nn_dot(low, v)) * (1.0 / share)).astype(BF16))

    @pl.when(y >= 2)
    def _():
        t3 = jnp.where(y == YN - 1, turned(taps[...]), taps[...])
        c = p_scr[:, :LANES].astype(BF16).astype(F32)
        p_scr[:, :LANES] = (c * turned(c)).astype(BF16).astype(F32)
        for b in range(YN):
            at = WINDOW + TOK * b
            before = p_scr[at - 1 : at - 1 + TOK, :LANES]
            here = p_scr[at : at + TOK, :LANES]
            after = p_scr[at + 1 : at + 1 + TOK, :LANES]
            post = p_scr[at : at + TOK, LANES:].astype(BF16).astype(F32)
            send(b, (post * (t3[0:1] * before + t3[1:2] * here + t3[2:3] * after)).astype(BF16))

    for b in range(YN):
        outgoing(b).wait()


def joined(a, b, left):
    return jnp.where(left, a, turned(b)), jnp.where(left, turned(a), b)


def gate_kernel(g_0, g_1, g_2, g_3, out, g_scr):
    y = lax.axis_index("y")
    for k, g in enumerate((g_0, g_1, g_2, g_3)):
        g_scr[k] = g[...]
    left = lax.broadcasted_iota(jnp.int32, (HALF, LANES), 1) < HALF
    for branch in range(2):
        parts = [g_scr[lax.rem(y + YN - source, YN)] for source in (2 * branch, 2 * branch + 1)]
        out[branch] = jax.nn.sigmoid(jnp.concatenate(joined(*parts, left), axis=0))


def partial_kernel(m, keep, give):
    first_core = lax.axis_index("c") == 0
    left = lax.broadcasted_iota(jnp.int32, (TOK, LANES), 1) < HALF
    for branch in range(2):
        mixed, even, odd = [], [], []
        for x in range(XN):
            a, b = m[YN * x + 2 * branch], m[YN * x + 2 * branch + 1]
            both = joined(a[:TOK], b[:TOK], left)
            mixed.append(both[0])
            even.append(both[1])
            odd.append(jnp.concatenate(joined(a[TOK:], b[TOK:], left[:HALF]), axis=0))
        mixed = jnp.concatenate(mixed, axis=1)
        sums = [nt_dot(mixed, jnp.concatenate(columns, axis=1)) for columns in (even, odd)]
        keep[branch] = jnp.where(first_core, sums[0], sums[1])
        give[branch] = jnp.where(first_core, sums[1], sums[0])


def final_kernel(keep, came, gates, out):
    other = 1 - lax.axis_index("c")
    total = jnp.zeros((TOK, LANES), F32)
    for branch in range(2):
        total = total + gates[branch] * (keep[branch] + came[other, branch])
    out[...] = total.astype(BF16)


VM = pl.BlockSpec(memory_space=pltpu.VMEM)


def shaped(shape, kind=BF16):
    return jax.ShapeDtypeStruct(shape, kind)


def call(kernel, outs, args, specs=None, scratch=(), limit=8, first=None):
    out_specs = jax.tree.map(lambda _: VM, outs)
    if first is not None:
        out_specs = (first,) + out_specs[1:]
    return pl.pallas_call(
        kernel,
        out_shape=outs,
        in_specs=specs or [VM] * len(args),
        out_specs=out_specs,
        scratch_shapes=list(scratch),
        compiler_params=pltpu.CompilerParams(vmem_limit_bytes=limit * 2**20),
    )(*args)


def on_device(tok, gain, q, k, v, ci, pre, post, ag, cg, sink, taps, wa, wc):
    plane = ("x", "c", "y")
    edges = [(YN * z + YN - 1, YN * z + YN) for z in range(ZN - 1)]
    edge = lax.ppermute(tok, ("z", "y"), edges + [(b, a) for a, b in edges])
    wy = call(pack_kernel, shaped((YN, 40, LANES)), (q, k, v, ci, pre, post, ag, cg, wa.T, wc.T), limit=60)
    wy = lax.all_to_all(wy, "y", 0, 0, tiled=True)
    spread = call(spread_kernel, shaped((PLANE, SLOT + 8, LANES)), (tok, gain.reshape(1, LANES), edge), limit=60)
    gathered_tok = lax.all_to_all(spread, plane, 0, 0, tiled=True)
    w = lax.all_gather(wy.reshape(YN * 40, LANES), "z", axis=0, tiled=True).reshape(ZN, YN, 40, LANES)
    message, *gates = call(
        mix_kernel,
        (shaped((XN, YN, TOK + HALF, LANES)),) + (shaped((HALF, LANES), F32),) * 4,
        (gathered_tok, w, taps, sink.reshape(1, 2)),
        [VM] * 4,
        [
            pltpu.VMEM((ROWS, FEATURES), BF16),
            pltpu.VMEM((ROWS, 2 * LANES), F32),
            pltpu.VMEM((YN, HALF, LANES), F32),
            pltpu.VMEM((TPN, LANES, LANES), BF16),
            pltpu.VMEM((XN, YN, TOK + HALF, LANES), BF16),
            pltpu.SemaphoreType.DMA((YN,)),
        ],
        20,
        first=pl.BlockSpec(memory_space=pl.ANY),
    )
    message = lax.all_to_all(message.reshape(XN * YN, TOK + HALF, LANES), ("x", "y"), 0, 0, tiled=True)
    for k in range(1, YN):
        gates[k] = lax.ppermute(gates[k], "y", [(y, (y + k) % YN) for y in range(YN)])
    gates = call(gate_kernel, shaped((2, TOK, LANES), F32), gates, scratch=[pltpu.VMEM((YN, HALF, LANES), F32)])
    sums = shaped((2, TOK, LANES), F32)
    keep, give = call(partial_kernel, (sums, sums), (message,))
    came = lax.all_gather(give, "c")
    return call(final_kernel, shaped((TOK, LANES)), (keep, came, gates))


def solution(mesh):
    finer = Mesh(mesh.devices.reshape(ZN, YN, XN, CN), ("z", "y", "x", "c"))
    sp, tp = ("z", "y"), ("x", "c")
    rows = P(sp, tp)
    columns = P(tp, sp)
    return jax.shard_map(
        on_device,
        mesh=finer,
        in_specs=(rows, P(tp)) + (rows,) * 8 + (P(tp), P(None, tp), columns, columns),
        out_specs=rows,
        check_vma=False,
    )
```

```python
import jax
import jax.numpy as jnp
from jax import lax
from jax.experimental import pallas as pl
from jax.experimental.pallas import tpu as pltpu
from jax.sharding import Mesh
from jax.sharding import PartitionSpec as P


ZN, YN, XN, CN = 16, 4, 4, 2
TPN = XN * CN
PLANE = YN * TPN
HALF = 64
WINDOW = 64
LANES = 128
TOK = 128
ROWS = YN * TOK + 2 * WINDOW
SLOT = TOK + WINDOW
FEATURES = TPN * LANES
EPSILON = 1e-06
NEGATIVE = -1e30
F32 = jnp.float32
BF16 = jnp.bfloat16


def nt_dot(a, b):
    return lax.dot_general(a, b, (((1,), (1,)), ((), ())), preferred_element_type=F32)


def nn_dot(a, b):
    return jnp.dot(a, b, preferred_element_type=F32)


def turned(block):
    return jnp.concatenate([block[:, HALF:], block[:, :HALF]], axis=1)


def pack_kernel(q, k, v, ci, pre, post, ag, cg, wa, wc, wy_out):
    for role in range(YN):
        half = slice(HALF * (role % 2), HALF * (role % 2) + HALF)
        first = (q, k, v) if role < 2 else (ci, pre, post)
        first = [block[:, half] if block.shape[1] == LANES else block[...] for block in first]
        gate, out_weight = (ag, wa) if role < 2 else (cg, wc)
        wy_out[role, 0:16, :] = jnp.concatenate(first[:2], axis=1)
        wy_out[role, 16:32, :] = jnp.concatenate([first[2], gate[:, half]], axis=1)
        rows = out_weight[:, half].astype(F32)
        wy_out[role, 32:40, :] = jnp.concatenate([rows[:8], rows[8:]], axis=1).astype(BF16)


def spread_kernel(tok, gain, edge, out):
    y = lax.axis_index("y")
    g = gain[...]
    high = g.astype(BF16)
    rest = g - high.astype(F32)
    middle = rest.astype(BF16)
    low = (rest - middle.astype(F32)).astype(BF16)
    row = lax.broadcasted_iota(jnp.int32, (8, LANES), 0)
    parts = [jnp.broadcast_to(part.astype(F32), (8, LANES)) for part in (high, middle, low)]
    gains = jnp.where(row == 0, parts[0], jnp.where(row == 1, parts[1], jnp.where(row == 2, parts[2], 0.0)))
    gains = gains.astype(BF16)
    block = tok[...]
    halo = jnp.where(y == YN - 1, edge[:WINDOW, :], edge[TOK - WINDOW :, :])
    for peer in range(PLANE):
        out[peer, :TOK, :] = block
        out[peer, TOK:SLOT, :] = halo
        out[peer, SLOT:, :] = gains


def mix_kernel(t, w, taps, sink, out, gate_0, gate_1, gate_2, gate_3, n_scr, p_scr, g_scr, w_scr, m_scr, sems):
    y = lax.axis_index("y")
    z = lax.axis_index("z")
    gains = []
    for tp in range(TPN):
        r = t[YN * tp, SLOT:, :].astype(F32)
        gains.append(r[0:1] + r[1:2] + r[2:3])
    segments = [(0, 0, TOK, WINDOW)]
    segments += [(WINDOW + TOK * b, b, 0, TOK) for b in range(YN)]
    segments += [(WINDOW + TOK * YN, YN - 1, TOK, WINDOW)]
    for at, b, start, count in segments:
        total = jnp.zeros((count, LANES), F32)
        for tp in range(TPN):
            x = t[YN * tp + b, start : start + count, :].astype(F32)
            total = total + x * x
        scale = lax.rsqrt(jnp.sum(total, axis=1, keepdims=True) / FEATURES + EPSILON)
        for tp in range(TPN):
            x = t[YN * tp + b, start : start + count, :].astype(F32)
            n_scr[at : at + count, LANES * tp : LANES * (tp + 1)] = (x * scale * gains[tp]).astype(BF16)
    weight = jnp.concatenate(
        [w[:, :, 16 * pair : 16 * pair + 16, :].reshape(FEATURES, LANES) for pair in range(2)], axis=1
    )
    p_scr[...] = nn_dot(n_scr[...], weight)
    left = lax.broadcasted_iota(jnp.int32, (TOK, LANES), 1) < HALF
    for b in range(YN):
        at = WINDOW + TOK * b
        g_scr[b] = jnp.where(left[:HALF], turned(p_scr[at : at + HALF, LANES:]), p_scr[at + HALF : at + TOK, LANES:])
    for k, gate in enumerate((gate_0, gate_1, gate_2, gate_3)):
        gate[...] = g_scr[lax.rem(y + k, YN)]

    for tp in range(TPN):
        rows = w[2 * tp : 2 * tp + 2, :, 32:40, :].astype(F32).reshape(TPN, 8, LANES)
        rows = jnp.stack([turned(rows.reshape(HALF, LANES)).reshape(TPN, 8, LANES), rows], axis=1)
        w_scr[tp] = rows.reshape(LANES, LANES).astype(BF16)

    for x in range(XN):
        packed = jnp.where(left[:HALF], turned(w_scr[2 * x + 1])[:HALF], w_scr[2 * x + 1][HALF:])
        for b in range(YN):
            m_scr[b, x, TOK:, :] = packed

    def outgoing(b):
        return pltpu.make_async_copy(m_scr.at[b], out.at[b], sems.at[b])

    def send(b, mixed):
        for x in range(XN):
            m_scr[b, x, :TOK, :] = jnp.where(left, mixed, w_scr[2 * x])
        outgoing(b).start()

    @pl.when(y < 2)
    def _():
        lane = lax.broadcasted_iota(jnp.int32, (1, 2), 1)
        logit = jnp.sum(jnp.where(lane == y, sink[...], 0.0), axis=1, keepdims=True)
        span = TOK + 2 * WINDOW
        i = lax.broadcasted_iota(jnp.int32, (TOK, span), 0)
        j = lax.broadcasted_iota(jnp.int32, (TOK, span), 1)
        near = jnp.abs(i + WINDOW - j) <= WINDOW
        edge_low, edge_high = jnp.where(z == 0, WINDOW, 0), jnp.where(z == ZN - 1, TOK + WINDOW, span)
        masks = [near & (j >= edge_low)] + [near] * (YN - 2) + [near & (j < edge_high)]
        scores, tops, weights = [], [], []
        for b in range(YN):
            q = p_scr[WINDOW + TOK * b : WINDOW + TOK * (b + 1), :HALF].astype(BF16)
            k = p_scr[TOK * b : TOK * b + span, HALF:LANES].astype(BF16)
            scores.append(jnp.where(masks[b], nt_dot(q, k) * (HALF**-0.5), NEGATIVE))
        for b in range(YN):
            tops.append(jnp.maximum(jnp.max(scores[b], axis=1, keepdims=True), logit))
        for b in range(YN):
            weights.append(jnp.exp(scores[b] - tops[b]))
        for b in range(YN):
            v = p_scr[TOK * b : TOK * b + span, LANES:].astype(BF16)
            share = jnp.sum(weights[b], axis=1, keepdims=True) + jnp.exp(logit - tops[b])
            high = weights[b].astype(BF16)
            low = (weights[b] - high.astype(F32)).astype(BF16)
            send(b, ((nn_dot(high, v) + nn_dot(low, v)) * (1.0 / share)).astype(BF16))

    @pl.when(y >= 2)
    def _():
        t3 = jnp.where(y == YN - 1, turned(taps[...]), taps[...])
        c = p_scr[:, :LANES].astype(BF16).astype(F32)
        p_scr[:, :LANES] = (c * turned(c)).astype(BF16).astype(F32)
        for b in range(YN):
            at = WINDOW + TOK * b
            before = p_scr[at - 1 : at - 1 + TOK, :LANES]
            here = p_scr[at : at + TOK, :LANES]
            after = p_scr[at + 1 : at + 1 + TOK, :LANES]
            post = p_scr[at : at + TOK, LANES:].astype(BF16).astype(F32)
            send(b, (post * (t3[0:1] * before + t3[1:2] * here + t3[2:3] * after)).astype(BF16))

    for b in range(YN):
        outgoing(b).wait()


def joined(a, b, left):
    return jnp.where(left, a, turned(b)), jnp.where(left, turned(a), b)


def gate_kernel(g_0, g_1, g_2, g_3, out, g_scr):
    y = lax.axis_index("y")
    for k, g in enumerate((g_0, g_1, g_2, g_3)):
        g_scr[k] = g[...]
    left = lax.broadcasted_iota(jnp.int32, (HALF, LANES), 1) < HALF
    for branch in range(2):
        parts = [g_scr[lax.rem(y + YN - source, YN)] for source in (2 * branch, 2 * branch + 1)]
        out[branch] = jax.nn.sigmoid(jnp.concatenate(joined(*parts, left), axis=0))


def partial_kernel(m, keep, give):
    first_core = lax.axis_index("c") == 0
    left = lax.broadcasted_iota(jnp.int32, (TOK, LANES), 1) < HALF
    for branch in range(2):
        mixed, even, odd = [], [], []
        for x in range(XN):
            a, b = m[2 * branch * XN + x], m[(2 * branch + 1) * XN + x]
            both = joined(a[:TOK], b[:TOK], left)
            mixed.append(both[0])
            even.append(both[1])
            odd.append(jnp.concatenate(joined(a[TOK:], b[TOK:], left[:HALF]), axis=0))
        mixed = jnp.concatenate(mixed, axis=1)
        sums = [nt_dot(mixed, jnp.concatenate(columns, axis=1)) for columns in (even, odd)]
        keep[branch] = jnp.where(first_core, sums[0], sums[1])
        give[branch] = jnp.where(first_core, sums[1], sums[0])


def final_kernel(keep, came, gates, out):
    other = 1 - lax.axis_index("c")
    total = jnp.zeros((TOK, LANES), F32)
    for branch in range(2):
        total = total + gates[branch] * (keep[branch] + came[other, branch])
    out[...] = total.astype(BF16)


VM = pl.BlockSpec(memory_space=pltpu.VMEM)


def shaped(shape, kind=BF16):
    return jax.ShapeDtypeStruct(shape, kind)


def call(kernel, outs, args, specs=None, scratch=(), limit=8, first=None):
    out_specs = jax.tree.map(lambda _: VM, outs)
    if first is not None:
        out_specs = (first,) + out_specs[1:]
    return pl.pallas_call(
        kernel,
        out_shape=outs,
        in_specs=specs or [VM] * len(args),
        out_specs=out_specs,
        scratch_shapes=list(scratch),
        compiler_params=pltpu.CompilerParams(vmem_limit_bytes=limit * 2**20),
    )(*args)


def on_device(tok, gain, q, k, v, ci, pre, post, ag, cg, sink, taps, wa, wc):
    plane = ("x", "c", "y")
    edges = [(YN * z + YN - 1, YN * z + YN) for z in range(ZN - 1)]
    edge = lax.ppermute(tok, ("z", "y"), edges + [(b, a) for a, b in edges])
    wy = call(pack_kernel, shaped((YN, 40, LANES)), (q, k, v, ci, pre, post, ag, cg, wa.T, wc.T), limit=60)
    wy = lax.all_to_all(wy, "y", 0, 0, tiled=True)
    spread = call(spread_kernel, shaped((PLANE, SLOT + 8, LANES)), (tok, gain.reshape(1, LANES), edge), limit=60)
    gathered_tok = lax.all_to_all(spread, plane, 0, 0, tiled=True)
    w = lax.all_gather(wy.reshape(YN * 40, LANES), "z", axis=0, tiled=True).reshape(ZN, YN, 40, LANES)
    message, *gates = call(
        mix_kernel,
        (shaped((YN, XN, TOK + HALF, LANES)),) + (shaped((HALF, LANES), F32),) * 4,
        (gathered_tok, w, taps, sink.reshape(1, 2)),
        [VM] * 4,
        [
            pltpu.VMEM((ROWS, FEATURES), BF16),
            pltpu.VMEM((ROWS, 2 * LANES), F32),
            pltpu.VMEM((YN, HALF, LANES), F32),
            pltpu.VMEM((TPN, LANES, LANES), BF16),
            pltpu.VMEM((YN, XN, TOK + HALF, LANES), BF16),
            pltpu.SemaphoreType.DMA((YN,)),
        ],
        20,
        first=pl.BlockSpec(memory_space=pl.ANY),
    )
    message = lax.all_to_all(message.reshape(YN * XN, TOK + HALF, LANES), ("y", "x"), 0, 0, tiled=True)
    for k in range(1, YN):
        gates[k] = lax.ppermute(gates[k], "y", [(y, (y + k) % YN) for y in range(YN)])
    gates = call(gate_kernel, shaped((2, TOK, LANES), F32), gates, scratch=[pltpu.VMEM((YN, HALF, LANES), F32)])
    sums = shaped((2, TOK, LANES), F32)
    keep, give = call(partial_kernel, (sums, sums), (message,))
    came = lax.all_gather(give, "c")
    return call(final_kernel, shaped((TOK, LANES)), (keep, came, gates))


def solution(mesh):
    finer = Mesh(mesh.devices.reshape(ZN, YN, XN, CN), ("z", "y", "x", "c"))
    sp, tp = ("z", "y"), ("x", "c")
    rows = P(sp, tp)
    columns = P(tp, sp)
    return jax.shard_map(
        on_device,
        mesh=finer,
        in_specs=(rows, P(tp)) + (rows,) * 8 + (P(tp), P(None, tp), columns, columns),
        out_specs=rows,
        check_vma=False,
    )
```
